512 devices in a mesh: ep: 32 (over z, x), tp: 16 (over y, core).
Axes of the slice: x: 4, y: 8, z: 8, core: 2. Of those that a mesh axis runs over, the one named last changes fastest.
Arguments:
- receptance: bfloat16 [8192, 1024], P('ep', 'tp'), may hold values from -6 to 6
- head_key_input: bfloat16 [8192, 1024], P('ep', 'tp'), may hold values from -12 to 12
- head_value_input: bfloat16 [8192, 1024], P('ep', 'tp'), may hold values from -6 to 6
- decay_input_part: bfloat16 [8192, 1024], P('ep', 'tp'), may hold values from -4 to 4
- learning_rate_input: bfloat16 [8192, 1024], P('ep', 'tp'), may hold values from -7 to 1
- output_gate_input: bfloat16 [8192, 1024], P('ep', 'tp'), may hold values from -6 to 6
- decay_channel_offset: float32 [1024], P('tp'), may hold values from -12.5 to -2
- spike_log_decay: float32 [8192, 1024], P('ep', 'tp'), may hold values from -0.7 to 0
- head_norm_gain: float32 [1024], P('tp'), may hold values from 0.1 to 1.9
- head_output_weight: bfloat16 [1024, 2048], P('tp'), may hold values from -0.25 to 0.25
- projection_norm_gain: float32 [2048], replicated, may hold values from 0.1 to 1.9
- expert_input_rows: bfloat16 [4096, 2048], P('ep'), may hold values from -6 to 6
- expert_norm_gain: float32 [2048], replicated, may hold values from 0.1 to 1.9
- selected_expert_index: int32 [4096, 2], P('ep'), may hold values from 0 to 255, all different within a row; in each aligned block of 128 rows (0 to 127, 128 to 255, ...) at most 2 rows name the same one
- selected_expert_weight: float32 [4096, 2], P('ep'), may hold values from 0.3 to 1.5
- routed_gate_weight: bfloat16 [512, 2048, 256], P(('ep', 'tp')), may hold values from -0.125 to 0.125
- routed_up_weight: bfloat16 [512, 2048, 256], P(('ep', 'tp')), may hold values from -0.125 to 0.125
- routed_down_weight: bfloat16 [512, 256, 2048], P(('ep', 'tp')), may hold values from -0.25 to 0.25
- common_gate_weight: bfloat16 [2048, 1024], P(None, 'tp'), may hold values from -0.125 to 0.125
- common_up_weight: bfloat16 [2048, 1024], P(None, 'tp'), may hold values from -0.125 to 0.125
- common_down_weight: bfloat16 [1024, 2048], P('tp'), may hold values from -0.25 to 0.25
Outputs:
- attention_output: bfloat16 [8192, 2048], P(('ep', 'tp'))
- expert_output: bfloat16 [4096, 2048], P('ep', 'tp')
The draws below stay inside these ranges and needn't reach their ends.
Inputs may be any that keep to these rules, and one draw needn't show every extreme that they name: `selected_expert_index`: each row names 2 different experts. Among the rows of one index of ep (aligned blocks of 128 rows) no expert is named by more than 2 rows, a bound that some block reaches.
All inputs are finite; a program needn't handle non-finite values.
Results may differ from the reference program's by a relative error of at most 0.023.
Values may be sent and summed in bfloat16 or wider, within the bound.
A program may use at most 64 MiB of HBM per device.

```python
import math
import jax
import jax.numpy as jnp
import numpy as np
from jax import lax

D = 2048
HEADS = 16
HEAD_CHANNELS = 64
FF = 512
SHARED_FF = 1024
TOPK = 2
TOK_A = 256
TOK_B = 128
WIDTH = 1024
EXPERTS = 256
CAP = 2
TOKENS_A = 8192
TOKENS_B = 4096
N_EP = 32
N_TP = 16


def draw_decay_channel_offset(key, part):
    head_key, fast_key, slow_key = jax.random.split(jax.random.fold_in(key, 11), 3)
    fast_share = 0.5
    fast_heads = jax.random.uniform(head_key, (HEADS,), jnp.float32) < fast_share
    fast_values = jax.random.uniform(fast_key, (WIDTH,), jnp.float32, minval=-3.0, maxval=-2.0)
    slow_values = jax.random.uniform(slow_key, (WIDTH,), jnp.float32, minval=-12.5, maxval=-11.0)
    fast_channels = jnp.repeat(fast_heads, HEAD_CHANNELS)
    return jnp.where(fast_channels, fast_values, slow_values).astype(jnp.float32)


def draw_spike_log_decay(key, part):
    spot_key, depth_key = jax.random.split(jax.random.fold_in(key, 23))
    struck = jax.random.uniform(spot_key, (TOKENS_A, HEADS), jnp.float32) < 3.0 / TOKENS_A
    depth = jax.random.uniform(depth_key, (TOKENS_A, HEADS), jnp.float32, minval=-0.7, maxval=-0.22)
    per_head = jnp.where(struck, depth, jnp.zeros_like(depth))
    return jnp.repeat(per_head, HEAD_CHANNELS, axis=1).astype(jnp.float32)


def draw_decay_input_part(key, part):
    noise_key, offset_key = jax.random.split(jax.random.fold_in(key, 37))
    groups = TOKENS_A // TOK_A
    noise = jax.random.normal(noise_key, (groups, TOK_A, WIDTH), jnp.float32) * 0.7
    offset = jax.random.uniform(offset_key, (groups, 1, 1), jnp.float32, minval=-0.8, maxval=0.8)
    values = jnp.clip(noise + offset, -4.0, 4.0).reshape(TOKENS_A, WIDTH)
    return values.astype(jnp.bfloat16)


def draw_head_key_input(key, part):
    common_key, noise_key = jax.random.split(jax.random.fold_in(key, 41))
    common = jnp.clip(jax.random.normal(common_key, (WIDTH,), jnp.float32), -2.7, 2.7) * 3.0
    noise = jnp.clip(jax.random.normal(noise_key, (TOKENS_A, WIDTH), jnp.float32), -3.5, 3.5)
    values = jnp.clip(common[None, :] + noise, -12.0, 12.0)
    return values.astype(jnp.bfloat16)


def draw_learning_rate_input(key, part):
    rate_key = jax.random.fold_in(key, 53)
    values = jax.random.normal(rate_key, (TOKENS_A, WIDTH), jnp.float32) - 3.0
    return jnp.clip(values, -7.0, 1.0).astype(jnp.bfloat16)


def strengthened(drawn, key, source, target, blocks, factor):
    owner, partner = [(jnp.arange(drawn.shape[position]) // (drawn.shape[position] // blocks)).reshape([-1 if axis == position else 1 for axis in range(drawn.ndim)]) for position in (source, target)]
    chosen = jax.random.permutation(key, blocks)[partner]
    strong = (owner == chosen) | (owner == (partner + blocks // 2) % blocks)
    return jnp.where(strong, factor * drawn, drawn)


def steps_of(stream_key, dims, cuts, least, top_value):
    def one(position, blocks):
        draws = jax.random.uniform(jax.random.fold_in(jax.random.fold_in(stream_key, 6), position), (blocks,), jnp.float32, least / len(cuts), top_value / len(cuts))
        return jnp.repeat(jnp.exp(draws), dims[position] // blocks).reshape((-1,) + (1,) * (len(dims) - position - 1))

    level = one(*cuts[0])
    for cut in cuts[1:]:
        level = level * one(*cut)
    return level


def assign_block(own_key, own, number, rows, number_of, top, reach, slope):
    order = jax.random.permutation(own_key, number_of)
    heavy_load, usual = portions_of(number_of, rows * top, reach, slope, True), portions_of(number_of, rows * top, reach, slope, False)
    places = jnp.arange(number_of)

    def named(tallies, offset_by):
        used = int((tallies > 0).sum())
        fixed = max(1, used // 4)
        moved = fixed + (places - fixed + offset_by * (used - fixed)) % max(1, number_of - fixed)
        return jnp.zeros((number_of,), jnp.int32).at[order[jnp.where(places < fixed, places, moved)]].set(jnp.asarray(tallies, jnp.int32))

    tallies = jnp.where(number % 4 == 0, named(heavy_load, number // 4), named(usual, number - number // 4 - 1))
    mixed = jax.random.permutation(jax.random.fold_in(own, 3), number_of)
    source_of, sink = mixed[0:number_of // 2 * 2:2], mixed[1:number_of // 2 * 2:2]
    room = jnp.minimum(tallies[source_of] - 1, reach - tallies[sink]) // 2
    room = jnp.where((source_of == order[0]) | (sink == order[0]) | (tallies[sink] == 0), 0, jnp.maximum(room, 0))
    moved = jax.random.randint(jax.random.fold_in(own, 4), (number_of // 2,), 0, 1 << 20) % (room + 1)
    tallies = tallies.at[source_of].add(-moved).at[sink].add(moved)
    labels = jnp.searchsorted(jnp.cumsum(tallies), jnp.arange(rows * top), side="right").astype(jnp.int32)
    listing = labels.reshape(top, rows).T
    listing = listing[jax.random.permutation(jax.random.fold_in(own, 1), rows)]
    offset_by = jax.random.randint(jax.random.fold_in(own, 2), (rows, 1), 0, top)
    return jnp.take_along_axis(listing, (jnp.arange(top)[None, :] + offset_by) % top, axis=1)


def portions_of(amount, total, limit, lean, full):
    weights = [(1 << 20) // math.isqrt(standing ** lean) + 1 for standing in range(1, amount + 1)]
    largest = limit if full else min(limit, max(-(-total // amount), total * weights[0] // sum(weights)))
    least = 1 if total - largest >= amount - 1 else 0
    holding, spare = [largest] + [least] * (amount - 1), total - largest - least * (amount - 1)
    while spare > 0:
        movable = [i for i in range(1, amount) if holding[i] < largest] or [i for i in range(1, amount) if holding[i] < limit]
        mass, left = sum([weights[i] for i in movable]), spare
        for i in movable:
            addition = min(limit - holding[i], max(1, left * weights[i] // mass), spare)
            holding[i] = holding[i] + addition
            spare = spare - addition
    return np.array(holding)


def scatter_about(own_key, shape, scale, reach, cuts=(), held_as=jnp.bfloat16):
    array = scale * jax.random.normal(own_key, shape, jnp.float32)
    if cuts:
        array = array * steps_of(own_key, shape, cuts, -0.22, 0.18)
    return jnp.clip(array, -reach, reach).astype(held_as)


def noise_with(stream_key, dims, spread, most, pieces, heavy, kind=jnp.bfloat16):
    result = spread * jax.random.normal(stream_key, dims, jnp.float32)
    if pieces:
        result = result * steps_of(stream_key, dims, pieces, -0.22, 0.18)
    return jnp.clip(strengthened(result, jax.random.fold_in(stream_key, 3), *heavy), -most, most).astype(kind)


def setup_inputs(seed: int = 0) -> dict:
    key_of = jax.random.split(jax.random.key(seed), 22)
    receptance = scatter_about(key_of[0], (TOKENS_A, WIDTH), 1.0, 6.0, ((0, 32), (1, 16)))
    head_key_input = draw_head_key_input(jax.random.fold_in(key_of[21], 71), 0)
    head_value_input = scatter_about(key_of[2], (TOKENS_A, WIDTH), 1.0, 6.0, ((0, 32), (1, 16)))
    decay_input_part = draw_decay_input_part(jax.random.fold_in(key_of[21], 71), 0)
    learning_rate_input = draw_learning_rate_input(jax.random.fold_in(key_of[21], 71), 0)
    output_gate_input = scatter_about(key_of[5], (TOKENS_A, WIDTH), 1.5, 6.0, ((0, 32), (1, 16)))
    decay_channel_offset = draw_decay_channel_offset(jax.random.fold_in(key_of[21], 71), 0)
    spike_log_decay = draw_spike_log_decay(jax.random.fold_in(key_of[21], 71), 0)
    head_norm_gain = jnp.clip(1.0 + 0.18 * jax.random.normal(key_of[8], (WIDTH,), jnp.float32), 0.1, 1.9)
    head_output_weight = noise_with(key_of[9], (WIDTH, D), WIDTH ** -0.5, 0.25, ((0, 16),), (0, 1, 16, 2.0))
    projection_norm_gain = jnp.clip(1.0 + 0.18 * jax.random.normal(key_of[10], (D,), jnp.float32), 0.1, 1.9)
    expert_input_rows = scatter_about(key_of[11], (TOKENS_B, D), 1.0, 6.0, ((0, 32),))
    expert_norm_gain = jnp.clip(1.0 + 0.18 * jax.random.normal(key_of[12], (D,), jnp.float32), 0.1, 1.9)
    selected_expert_index_keys = jax.random.split(jax.random.fold_in(key_of[13], 1), TOKENS_B // TOK_B)
    selected_expert_index_turns = jax.random.permutation(jax.random.fold_in(key_of[13], 3), TOKENS_B // TOK_B)
    selected_expert_index = jax.vmap(lambda own, number: assign_block(jax.random.fold_in(key_of[13], 2), own, number, TOK_B, EXPERTS, TOPK, CAP, 1))(selected_expert_index_keys, selected_expert_index_turns).reshape((TOKENS_B, TOPK))
    selected_expert_weight = jnp.clip(0.3 + 1.2 * jax.random.uniform(key_of[14], (TOKENS_B, TOPK), jnp.float32) ** steps_of(key_of[14], (TOKENS_B, TOPK), ((0, 32),), -0.2, 0.2), 0.3, 1.5)
    routed_gate_weight = scatter_about(key_of[15], (2 * EXPERTS, D, FF // 2), D ** -0.5, 0.125, ((0, 512),))
    routed_up_weight = scatter_about(key_of[16], (2 * EXPERTS, D, FF // 2), D ** -0.5, 0.125, ((0, 512),))
    routed_down_weight = scatter_about(key_of[17], (2 * EXPERTS, FF // 2, D), FF ** -0.5, 0.25, ((0, 512),))
    common_gate_weight = scatter_about(key_of[18], (D, SHARED_FF), D ** -0.5, 0.125, ((1, 16),))
    common_up_weight = scatter_about(key_of[19], (D, SHARED_FF), D ** -0.5, 0.125, ((1, 16),))
    common_down_weight = noise_with(key_of[20], (SHARED_FF, D), SHARED_FF ** -0.5, 0.25, ((0, 16),), (0, 1, 16, 2.0))
    return dict(receptance=receptance, head_key_input=head_key_input, head_value_input=head_value_input, decay_input_part=decay_input_part, learning_rate_input=learning_rate_input, output_gate_input=output_gate_input, decay_channel_offset=decay_channel_offset, spike_log_decay=spike_log_decay, head_norm_gain=head_norm_gain, head_output_weight=head_output_weight, projection_norm_gain=projection_norm_gain, expert_input_rows=expert_input_rows, expert_norm_gain=expert_norm_gain, selected_expert_index=selected_expert_index, selected_expert_weight=selected_expert_weight, routed_gate_weight=routed_gate_weight, routed_up_weight=routed_up_weight, routed_down_weight=routed_down_weight, common_gate_weight=common_gate_weight, common_up_weight=common_up_weight, common_down_weight=common_down_weight)


FULL_PRECISION = lax.Precision.HIGHEST
NORM_EPSILON = 1e-06
GROUP_EPSILON = 0.00064

def rms_scale(values, gain):
    values = values.astype(jnp.float32)
    return values * lax.rsqrt(lax.optimization_barrier(jnp.mean(values * values, axis=-1, keepdims=True)) + NORM_EPSILON) * gain.astype(jnp.float32)

def blocked_down(hidden, weight):
    block_width = hidden.shape[1] // N_TP
    summed = jnp.zeros((hidden.shape[0], weight.shape[1]), jnp.float32)
    for block_index in range(N_TP):
        lower = block_index * block_width
        upper = lower + block_width
        partial_value = jnp.dot(hidden[:, lower:upper], weight[lower:upper], preferred_element_type=jnp.float32).astype(jnp.bfloat16)
        partial_value = lax.optimization_barrier(partial_value)
        summed = summed + partial_value.astype(jnp.float32)
    return summed

def attention_mixer(receptance, head_key_input, head_value_input, decay_input_part, learning_rate_input, output_gate_input, decay_channel_offset, spike_log_decay, head_norm_gain, head_output_weight, projection_norm_gain):
    sequence_length, width = receptance.shape
    number_of_heads = width // HEAD_CHANNELS

    def split_heads(values):
        return values.astype(jnp.float32).reshape(sequence_length, number_of_heads, HEAD_CHANNELS)
    recept = split_heads(receptance)
    keys = split_heads(head_key_input)
    values = split_heads(head_value_input)
    learn_rate = jax.nn.sigmoid(split_heads(learning_rate_input))
    decay_preactivation = decay_channel_offset.astype(jnp.float32)[None, :] + jnp.tanh(decay_input_part.astype(jnp.float32))
    decay_factor = jnp.exp(spike_log_decay.astype(jnp.float32) - jnp.exp(-jax.nn.softplus(-decay_preactivation) - 0.5)).reshape(sequence_length, number_of_heads, HEAD_CHANNELS)
    removal = keys * lax.rsqrt(lax.optimization_barrier(jnp.sum(keys * keys, axis=-1, keepdims=True)) + NORM_EPSILON)
    insertion = keys * learn_rate
    scaled_removal = removal * learn_rate

    def advance(state, inputs):
        recept_now, decay_now, insert_now, value_now, removal_now, scaled_now = inputs
        along = jnp.einsum('hvk,hk->hv', state, removal_now, precision=FULL_PRECISION)
        state = state * decay_now[:, None, :] - along[:, :, None] * scaled_now[:, None, :] + value_now[:, :, None] * insert_now[:, None, :]
        return (state, jnp.einsum('hvk,hk->hv', state, recept_now, precision=FULL_PRECISION))
    start = jnp.zeros((number_of_heads, HEAD_CHANNELS, HEAD_CHANNELS), jnp.float32)
    _, head_value = lax.scan(advance, start, (recept, decay_factor, insertion, values, removal, scaled_removal))
    centred = head_value - lax.optimization_barrier(jnp.mean(head_value, axis=-1, keepdims=True))
    normed = centred * lax.rsqrt(lax.optimization_barrier(jnp.mean(centred * centred, axis=-1, keepdims=True)) + GROUP_EPSILON)
    gated = normed.reshape(sequence_length, width) * head_norm_gain.astype(jnp.float32) * jax.nn.sigmoid(output_gate_input.astype(jnp.float32))
    heads_out = gated.astype(jnp.bfloat16)
    mix_sum = blocked_down(heads_out, head_output_weight)
    return rms_scale(mix_sum, projection_norm_gain).astype(jnp.bfloat16)

def expert_half(expert_input_rows, expert_norm_gain, selected_expert_index, selected_expert_weight, routed_gate_weight, routed_up_weight, routed_down_weight, common_gate_weight, common_up_weight, common_down_weight):
    normed = rms_scale(expert_input_rows, expert_norm_gain).astype(jnp.bfloat16)
    shared_hidden = (jax.nn.silu(jnp.dot(normed, common_gate_weight, preferred_element_type=jnp.float32)) * jnp.dot(normed, common_up_weight, preferred_element_type=jnp.float32)).astype(jnp.bfloat16)
    shared_sum = blocked_down(shared_hidden, common_down_weight)
    most_rows = N_EP * CAP

    def per_expert(summed, expert):
        hits = selected_expert_index == expert
        chosen = jnp.any(hits, axis=1)
        weight = lax.optimization_barrier(jnp.sum(jnp.where(hits, selected_expert_weight, jnp.zeros_like(selected_expert_weight)), axis=1))
        order = jnp.argsort(jnp.where(chosen, 0, 1).astype(jnp.int32), stable=True)[:most_rows].astype(jnp.int32)
        picked = normed[order]
        first_half = (2 * expert).astype(jnp.int32)
        gate_pair = lax.dynamic_slice_in_dim(routed_gate_weight, first_half, 2, 0)
        up_pair = lax.dynamic_slice_in_dim(routed_up_weight, first_half, 2, 0)
        down_pair = lax.dynamic_slice_in_dim(routed_down_weight, first_half, 2, 0)
        value = jnp.zeros((most_rows, normed.shape[1]), jnp.float32)
        for half in range(2):
            gate = jnp.dot(picked, gate_pair[half], preferred_element_type=jnp.float32)
            upward = jnp.dot(picked, up_pair[half], preferred_element_type=jnp.float32)
            hidden = (jax.nn.silu(gate) * upward).astype(jnp.bfloat16)
            partial_value = jnp.dot(hidden, down_pair[half], preferred_element_type=jnp.float32).astype(jnp.bfloat16)
            partial_value = lax.optimization_barrier(partial_value)
            value = value + partial_value.astype(jnp.float32)
        value = value.astype(jnp.bfloat16)
        value = lax.optimization_barrier(value)
        summed = summed.at[order].add(weight[order][:, None] * value.astype(jnp.float32))
        return (summed, None)
    start = jnp.zeros((expert_input_rows.shape[0], expert_input_rows.shape[1]), jnp.float32)
    routed, _ = lax.scan(per_expert, start, jnp.arange(EXPERTS, dtype=jnp.int32))
    return (routed + shared_sum).astype(jnp.bfloat16)

def reference(receptance, head_key_input, head_value_input, decay_input_part, learning_rate_input, output_gate_input, decay_channel_offset, spike_log_decay, head_norm_gain, head_output_weight, projection_norm_gain, expert_input_rows, expert_norm_gain, selected_expert_index, selected_expert_weight, routed_gate_weight, routed_up_weight, routed_down_weight, common_gate_weight, common_up_weight, common_down_weight):
    attention_output = attention_mixer(receptance, head_key_input, head_value_input, decay_input_part, learning_rate_input, output_gate_input, decay_channel_offset, spike_log_decay, head_norm_gain, head_output_weight, projection_norm_gain)
    expert_output = expert_half(expert_input_rows, expert_norm_gain, selected_expert_index, selected_expert_weight, routed_gate_weight, routed_up_weight, routed_down_weight, common_gate_weight, common_up_weight, common_down_weight)
    return (attention_output, expert_output)
```

```python
import functools
import math

import jax
import jax.numpy as jnp
from jax import lax
from jax.experimental import pallas as pl
from jax.experimental.pallas import tpu as pltpu
from jax.sharding import PartitionSpec as P

HC = 64
L = 128
GROUPS = 8
CAP = 2
NORM_EPSILON = 1e-06
GROUP_EPSILON = 0.00064
F32 = jnp.float32
BF16 = jnp.bfloat16
MESH = pl.DeviceIdType.MESH


def nn(a, b):
    return jnp.dot(a, b, preferred_element_type=F32)


def nt(a, b):
    return lax.dot_general(a, b, (((1,), (1,)), ((), ())), preferred_element_type=F32)


def parts(a, count):
    out = []
    for k in range(count):
        piece = a.astype(BF16)
        out.append(piece)
        if k < count - 1:
            a = a - piece.astype(F32)
    return out


def mm(a, b, product=nn, na=2, nb=2):
    pa = [a] if a.dtype == BF16 else parts(a, na)
    pb = [b] if b.dtype == BF16 else parts(b, nb)
    total = None
    for i, x in enumerate(pa):
        for j, y in enumerate(pb):
            if i + j < max(len(pa), len(pb)):
                term = product(x, y)
                total = term if total is None else total + term
    return total


def iota(shape, dim):
    return lax.broadcasted_iota(jnp.int32, shape, dim)


def sigmoid(v):
    return 1.0 / (1.0 + jnp.exp(-v))


def column(row):
    n = row.shape[1]
    return jnp.sum(
        jnp.where(iota((n, n), 0) == iota((n, n), 1), row, 0.0), axis=1, keepdims=True
    )


def beside_identity(f):
    top = jnp.where(iota((HC, 2 * HC), 0) == iota((HC, 2 * HC), 1), 1.0, 0.0)
    return jnp.concatenate([top.astype(f.dtype), f], axis=0)


def joined(late, early):
    return mm(late, beside_identity(early))


def block_inverse(n):
    r, c = iota((L, L), 0), iota((L, L), 1)
    eye = jnp.where(r == c, 1.0, 0.0)
    small = jnp.where(r // 8 == c // 8, n, 0.0)
    two = mm(small, small)
    four = mm(two, two)
    first = eye + small + two + mm(small, two)
    x = first + mm(first, four)
    size = 8
    while size < L:
        lower, upper = r // size, c // size
        off = jnp.where((upper == lower + 1) & (lax.rem(lower, 2) == 0), n, 0.0)
        x = x + mm(mm(x, off), x)
        size *= 2
    return x


def local_block(rec, key, val, removal, lr, ld):
    s, t = iota((L, L), 0), iota((L, L), 1)
    upto = jnp.where(s <= t, 1.0, 0.0).astype(BF16)
    cum = sum(nn(p, upto) for p in parts(ld, 3))
    ref, end = cum[:, L // 2 - 1 : L // 2], cum[:, L - 1 : L]
    eq = jnp.exp(cum - ref)
    eb = jnp.exp(cum - ld - ref)
    ek = jnp.exp(ref - cum)
    eref, eend = jnp.exp(ref), jnp.exp(end - ref)
    qn, qr = -removal * eb, rec * eq
    kb, kk = removal * lr * ek, key * lr * ek
    keys = jnp.concatenate([kb.T, kk.T], axis=0)
    both = mm(keys, jnp.concatenate([qn, qr], axis=1))
    lb = jnp.where(s < t, both[:L, :L], 0.0)
    ob = jnp.where(s <= t, both[:L, L:], 0.0)
    lk = jnp.where(s < t, both[L:, :L], 0.0)
    ok = jnp.where(s <= t, both[L:, L:], 0.0)
    valued = mm(val, jnp.concatenate([lk, ok], axis=1))
    right = jnp.concatenate([valued[:, :L], qn * eref], axis=0)
    corr = mm(right, block_inverse(lb))
    z = mm(corr, ob) + jnp.concatenate([valued[:, L:], qr * eref], axis=0)
    aug = jnp.concatenate([val, jnp.zeros_like(val)], axis=0)
    f = mm(
        jnp.concatenate([kb * eend, kk * eend], axis=1),
        jnp.concatenate([corr, aug.astype(F32)], axis=1),
        nt,
    )
    f = f + jnp.where(
        iota((HC, 2 * HC), 0) + HC == iota((HC, 2 * HC), 1), jnp.exp(end), 0.0
    )
    return f, z


def kernel(nx, nz, *refs):
    (rec, key, val, dec, lrn, gat, spk, dco, hng, png, eng, idx, wts) = refs[:13]
    (how_h, exr_h, rg_h, ru_h, rd_h, cg_h, cu_h, cd_h) = refs[13:21]
    out_a, out_b = refs[21:23]
    (how, exr, rg, ru, rd, cgu, cd, nb, dout, darr, ep, epr, es, rb, rout, rarr,
     sp, spr, ss, sb, ap, apr, aps, ab, xarr, zs, zarr, load, pair_s, pair_r, dsend, drecv,
     ysend, yrecv, rsend, rrecv, xsend, xrecv, zsend, zrecv) = refs[23:]
    n_ep = nx * nz
    tb = exr.shape[0]
    rows = n_ep * CAP
    slots = rows * GROUPS
    me, t = lax.axis_index("ep"), lax.axis_index("tp")
    y, c = lax.div(t, 2), lax.rem(t, 2)
    z, x = lax.div(me, nx), lax.rem(me, nx)
    other = t + 1 - 2 * c

    def remote(src, dst, send, recv, where):
        return pltpu.make_async_remote_copy(
            src_ref=src, dst_ref=dst, send_sem=send, recv_sem=recv,
            device_id=where, device_id_type=MESH,
        )

    def drain(ref, sem):
        pltpu.make_async_copy(ref, ref, sem).wait()

    loads = [
        pltpu.make_async_copy(a, b, load.at[k])
        for k, (a, b) in enumerate((
            (exr_h, exr), (cg_h, cgu.at[0:HC]), (cu_h, cgu.at[HC : 2 * HC]), (cd_h, cd),
            (rg_h, rg), (ru_h, ru), (rd_h, rd), (how_h, how),
        ))
    ]
    for copy in loads:
        copy.start()

    unit = jnp.where(iota((HC, 2 * HC), 0) + HC == iota((HC, 2 * HC), 1), 1.0, 0.0)
    for k in range(nz):
        zarr[k] = unit.astype(BF16)

    barrier = pltpu.get_barrier_semaphore()
    pl.semaphore_signal(barrier, inc=1, device_id={"tp": other}, device_id_type=MESH)
    for d in range(1, GROUPS):
        pl.semaphore_signal(
            barrier, inc=1, device_id={"tp": 2 * lax.rem(y + d, GROUPS) + c}, device_id_type=MESH
        )

    def greet(d, carry):
        pl.semaphore_signal(
            barrier, inc=1, device_id={"ep": lax.rem(me + d, n_ep)}, device_id_type=MESH
        )
        return carry

    lax.fori_loop(1, n_ep, greet, 0)

    loads[0].wait()
    wide = exr[...].astype(F32)
    scale = lax.rsqrt(jnp.mean(wide * wide, axis=1, keepdims=True) + NORM_EPSILON)
    nb[...] = (wide * scale * eng[...]).astype(BF16)

    width = nb.shape[1] // GROUPS
    first, second = idx[0:1, :], idx[1:2, :]
    i = iota((slots, tb), 0)
    expert = lax.div(i, 16) * GROUPS + y
    hits = jnp.where((first == expert) | (second == expert), 1.0, 0.0)
    earlier = jnp.where(iota((tb, tb), 0) < iota((tb, tb), 1), 1.0, 0.0).astype(BF16)
    rank = nn(hits.astype(BF16), earlier)
    mine = jnp.where(rank == lax.rem(lax.div(i, 8), 2).astype(F32), hits, 0.0)
    piece = lax.rem(i, 8)
    picks = jnp.concatenate(
        [jnp.where(piece == j, mine, 0.0).astype(BF16) for j in range(GROUPS)], axis=1
    )
    stacked = jnp.concatenate(
        [nb[:, j * width : (j + 1) * width] for j in range(GROUPS)], axis=0
    )
    dout[...] = nn(picks, stacked).astype(BF16)
    own = pl.ds(pl.multiple_of(me * 16, 16), 16)
    darr[own, :] = dout[own, :]

    loads[1].wait()
    loads[2].wait()
    loads[3].wait()
    gate_up = nt(cgu[...], nb[...])
    g, u = gate_up[:HC], gate_up[HC:]
    hidden = (g * sigmoid(g) * u).T.astype(BF16)
    shared = nn(hidden, cd[...]).astype(BF16)
    cols = shared.shape[1] // (2 * GROUPS)
    for k in range(2 * GROUPS):
        sp[k % 2, k // 2] = shared[:, k * cols : (k + 1) * cols]

    pl.semaphore_wait(barrier, GROUPS + n_ep - 1)

    def send_rows(d, carry):
        to = lax.rem(me + d, n_ep)
        remote(
            dout.at[pl.ds(pl.multiple_of(to * 16, 16), 16)], darr.at[own],
            dsend, drecv, {"ep": to},
        ).start()
        return carry

    lax.fori_loop(1, n_ep, send_rows, 0)
    pair_shared = remote(sp.at[1 - c], spr, pair_s.at[0], pair_r.at[0], {"tp": other})
    pair_shared.start()

    k_in = key[...].astype(F32)
    pre = column(dco[...]) + jnp.tanh(dec[...].astype(F32))
    ld = spk[...] - sigmoid(pre) * math.exp(-0.5)
    lr = sigmoid(lrn[...].astype(F32))
    removal = k_in * lax.rsqrt(jnp.sum(k_in * k_in, axis=0, keepdims=True) + NORM_EPSILON)
    r_in = rec[...].astype(F32)
    blocks = []
    for b in range(key.shape[1] // L):
        at = slice(b * L, (b + 1) * L)
        blocks.append(
            local_block(r_in[:, at], k_in[:, at], val[:, at], removal[:, at], lr[:, at], ld[:, at])
        )
    f, z_out = blocks[0]
    z_all = [z_out]
    for later_f, later_z in blocks[1:]:
        z_all.append(mm(beside_identity(f).T, later_z))
        f = joined(later_f, f)
    z_all = jnp.concatenate(z_all, axis=1)
    xarr[x] = f.astype(BF16)
    x_sends = [
        remote(
            xarr.at[x], xarr.at[x], xsend.at[d - 1], xrecv.at[d - 1],
            {"ep": z * nx + lax.rem(x + d, nx)},
        )
        for d in range(1, nx)
    ]
    for copy in x_sends:
        copy.start()

    pair_shared.wait()
    ss[...] = (sp[c].astype(F32) + spr[...].astype(F32)).astype(BF16)
    sb[y] = ss[y]
    y_sends = []
    for d in range(1, GROUPS):
        to = lax.rem(y + d, GROUPS)
        y_sends.append(
            remote(ss.at[to], sb.at[y], ysend.at[0, d - 1], yrecv.at[0, d - 1], {"tp": 2 * to + c})
        )
        y_sends[-1].start()

    drain(darr.at[0 : (n_ep - 1) * 16], drecv)
    r, q = iota((slots, slots), 0), iota((slots, slots), 1)
    source = lax.rem(r, n_ep) * 16 + lax.rem(lax.div(r, n_ep), 2) * 8 + lax.div(r, rows)
    turned = nn(jnp.where(q == source, 1.0, 0.0).astype(BF16), darr[...]).astype(BF16)
    rows_in = jnp.concatenate(
        [turned[j * rows : (j + 1) * rows] for j in range(GROUPS)], axis=1
    )
    loads[4].wait()
    loads[5].wait()
    g, u = nn(rows_in, rg[...]), nn(rows_in, ru[...])
    hidden = (g * sigmoid(g) * u).astype(BF16)
    loads[6].wait()
    routed = nn(hidden, rd[...]).astype(BF16)
    for k in range(2 * GROUPS):
        ep[k % 2, k // 2] = routed[:, k * cols : (k + 1) * cols]
    pair_routed = remote(ep.at[1 - c], epr, pair_s.at[1], pair_r.at[1], {"tp": other})
    pair_routed.start()

    for copy in x_sends:
        copy.wait()
    stretch = [xarr[k] for k in range(nx)]
    before = unit
    total = stretch[0]
    for k in range(1, nx):
        before = jnp.where(x == k, total.astype(F32), before)
        total = joined(stretch[k], total)
    zs[...] = total.astype(BF16)
    for d in range(1, nz):
        @pl.when(z + d < nz)
        def _():
            remote(
                zs, zarr.at[z], zsend.at[d - 1], zrecv.at[z], {"ep": (z + d) * nx + x}
            ).start()

    pair_routed.wait()
    es[...] = (ep[c].astype(F32) + epr[...].astype(F32)).astype(BF16)
    rb[y] = es[y]
    for d in range(1, GROUPS):
        to = lax.rem(y + d, GROUPS)
        y_sends.append(
            remote(es.at[to], rb.at[y], ysend.at[1, d - 1], yrecv.at[1, d - 1], {"tp": 2 * to + c})
        )
        y_sends[-1].start()
    z_all = mm(beside_identity(before).T, z_all)

    q = iota((slots, slots), 1)
    r = iota((slots, slots), 0)
    source = lax.div(lax.rem(r, 16), 2) * rows + lax.rem(r, 2) * n_ep + lax.div(r, 16)
    back = jnp.where(q == source, 1.0, 0.0).astype(BF16)
    lines = jnp.concatenate(
        [first.astype(F32), second.astype(F32), wts[...], jnp.zeros((4, tb), F32)], axis=0
    ).T
    q = iota((tb, slots), 1)
    expert = (lax.div(q, 16) * GROUPS + lax.div(lax.rem(q, 16), 2)).astype(F32)
    hit_a = jnp.where(lines[:, 0:1] == expert, 1.0, 0.0)
    hit_b = jnp.where(lines[:, 1:2] == expert, 1.0, 0.0)
    earlier = jnp.where(iota((tb, tb), 0) > iota((tb, tb), 1), 1.0, 0.0).astype(BF16)
    rank = nn(earlier, (hit_a + hit_b).astype(BF16))
    weight = jnp.where(
        rank == lax.rem(q, 2).astype(F32), hit_a * lines[:, 2:3] + hit_b * lines[:, 3:4], 0.0
    )

    for copy in y_sends[GROUPS - 1 :]:
        copy.wait()
    every = jnp.concatenate([rb[k] for k in range(GROUPS)], axis=0)
    rout[...] = nn(back, every).astype(BF16)
    rarr[own, :] = rout[own, :]

    def send_back(d, carry):
        to = lax.rem(me + d, n_ep)
        remote(
            rout.at[pl.ds(pl.multiple_of(to * 16, 16), 16)], rarr.at[own],
            rsend, rrecv, {"ep": to},
        ).start()
        return carry

    lax.fori_loop(1, n_ep, send_back, 0)

    for k in range(nz - 1):
        @pl.when(k < z)
        def _():
            drain(zarr.at[k], zrecv.at[k])

    level = [zarr[k] for k in range(nz - 1)] if nz > 1 else [unit.astype(BF16)]
    while len(level) > 1:
        nxt = [joined(level[k + 1], level[k]) for k in range(0, len(level) - 1, 2)]
        if len(level) % 2:
            nxt.append(level[-1].astype(F32))
        level = nxt
    carried = level[0].astype(F32)
    head = mm(beside_identity(carried).T[:HC], z_all)
    centred = head - jnp.mean(head, axis=0, keepdims=True)
    normed = centred * lax.rsqrt(jnp.mean(centred * centred, axis=0, keepdims=True) + GROUP_EPSILON)
    heads_out = normed * column(hng[...]) * sigmoid(gat[...].astype(F32))
    heads_out = heads_out.T.astype(BF16)
    loads[7].wait()
    mixed = nn(heads_out, how[...]).astype(BF16)
    own_rows = out_a.shape[0]
    for k in range(2 * GROUPS):
        ap[k % 2, k // 2] = mixed[k * own_rows : (k + 1) * own_rows]
    pair_mix = remote(ap.at[1 - c], apr, pair_s.at[2], pair_r.at[2], {"tp": other})
    pair_mix.start()
    pair_mix.wait()
    aps[...] = (ap[c].astype(F32) + apr[...].astype(F32)).astype(BF16)
    ab[y] = aps[y]
    a_sends = []
    for d in range(1, GROUPS):
        to = lax.rem(y + d, GROUPS)
        a_sends.append(
            remote(aps.at[to], ab.at[y], ysend.at[2, d - 1], yrecv.at[2, d - 1], {"tp": 2 * to + c})
        )
        a_sends[-1].start()

    for copy in y_sends[: GROUPS - 1]:
        copy.wait()
    drain(rarr.at[0 : (n_ep - 1) * 16], rrecv)
    answer = mm(weight, rarr[...])
    for k in range(GROUPS):
        answer = answer + sb[k].astype(F32)
    out_b[...] = answer.astype(BF16)

    for copy in a_sends:
        copy.wait()
    mix = ab[0].astype(F32)
    for k in range(1, GROUPS):
        mix = mix + ab[k].astype(F32)
    scale = lax.rsqrt(jnp.mean(mix * mix, axis=1, keepdims=True) + NORM_EPSILON)
    out_a[...] = (mix * scale * png[...]).astype(BF16)

    for d in range(1, nz):
        @pl.when(z + d < nz)
        def _():
            drain(zs, zsend.at[d - 1])
    drain(dout.at[0 : (n_ep - 1) * 16], dsend)
    drain(rout.at[0 : (n_ep - 1) * 16], rsend)


def solution(mesh):
    n_ep = mesh.shape["ep"]
    nx = 4 if n_ep % 4 == 0 else n_ep
    nz = n_ep // nx

    def body(rec, key, val, dec, lrn, gat, dco, spk, hng, how, png, exr, eng, idx, wts,
             rg, ru, rd, cg, cu, cd):
        ta, d = rec.shape[0], how.shape[1]
        tb = exr.shape[0]
        own, cols = ta // (2 * GROUPS), d // (2 * GROUPS)
        rows = n_ep * CAP
        width = d // GROUPS
        small = [a.T for a in (rec, key, val, dec, lrn, gat, spk)]
        small += [a.reshape(1, -1) for a in (dco, hng, png, eng)] + [idx.T, wts.T]
        large = [how, exr, rg[0], ru[0], rd[0], cg.T, cu.T, cd]
        vmem = pl.BlockSpec(memory_space=pltpu.VMEM)
        dma = pltpu.SemaphoreType.DMA
        return pl.pallas_call(
            functools.partial(kernel, nx, nz),
            out_shape=(
                jax.ShapeDtypeStruct((own, d), BF16),
                jax.ShapeDtypeStruct((tb, cols), BF16),
            ),
            in_specs=[vmem] * len(small) + [pl.BlockSpec(memory_space=pl.ANY)] * len(large),
            out_specs=(vmem, vmem),
            scratch_shapes=[
                pltpu.VMEM(how.shape, BF16),
                pltpu.VMEM(exr.shape, BF16),
                pltpu.VMEM(rg.shape[1:], BF16),
                pltpu.VMEM(ru.shape[1:], BF16),
                pltpu.VMEM(rd.shape[1:], BF16),
                pltpu.VMEM((2 * HC, d), BF16),
                pltpu.VMEM(cd.shape, BF16),
                pltpu.VMEM((tb, d), BF16),
                pltpu.VMEM((n_ep * 16, width), BF16),
                pltpu.VMEM((n_ep * 16, width), BF16),
                pltpu.VMEM((2, GROUPS, rows, cols), BF16),
                pltpu.VMEM((GROUPS, rows, cols), BF16),
                pltpu.VMEM((GROUPS, rows, cols), BF16),
                pltpu.VMEM((GROUPS, rows, cols), BF16),
                pltpu.VMEM((n_ep * 16, cols), BF16),
                pltpu.VMEM((n_ep * 16, cols), BF16),
                pltpu.VMEM((2, GROUPS, tb, cols), BF16),
                pltpu.VMEM((GROUPS, tb, cols), BF16),
                pltpu.VMEM((GROUPS, tb, cols), BF16),
                pltpu.VMEM((GROUPS, tb, cols), BF16),
                pltpu.VMEM((2, GROUPS, own, d), BF16),
                pltpu.VMEM((GROUPS, own, d), BF16),
                pltpu.VMEM((GROUPS, own, d), BF16),
                pltpu.VMEM((GROUPS, own, d), BF16),
                pltpu.VMEM((nx, HC, 2 * HC), BF16),
                pltpu.VMEM((HC, 2 * HC), BF16),
                pltpu.VMEM((nz, HC, 2 * HC), BF16),
                dma((8,)),
                dma((3,)),
                dma((3,)),
                dma,
                dma,
                dma((3, GROUPS - 1)),
                dma((3, GROUPS - 1)),
                dma,
                dma,
                dma((max(nx - 1, 1),)),
                dma((max(nx - 1, 1),)),
                dma((max(nz - 1, 1),)),
                dma((max(nz, 1),)),
            ],
            compiler_params=pltpu.CompilerParams(
                collective_id=0, has_side_effects=True, vmem_limit_bytes=48 * 1024 * 1024
            ),
        )(*small, *large)

    placed = (
        P("ep", "tp"), P("ep", "tp"), P("ep", "tp"), P("ep", "tp"), P("ep", "tp"), P("ep", "tp"),
        P("tp"), P("ep", "tp"), P("tp"), P("tp", None), P(), P("ep", None), P(), P("ep", None),
        P("ep", None), P(("ep", "tp"), None, None), P(("ep", "tp"), None, None),
        P(("ep", "tp"), None, None), P(None, "tp"), P(None, "tp"), P("tp", None),
    )
    return jax.shard_map(
        body,
        mesh=mesh,
        in_specs=placed,
        out_specs=(P(("ep", "tp"), None), P("ep", "tp")),
        check_vma=False,
    )
```

```python
import functools
import math

import jax
import jax.numpy as jnp
from jax import lax
from jax.experimental import pallas as pl
from jax.experimental.pallas import tpu as pltpu
from jax.sharding import PartitionSpec as P

HC = 64
L = 128
GROUPS = 8
CAP = 2
FAR_FIRST = (4, 3, 5, 2, 6, 1, 7)
NORM_EPSILON = 1e-06
GROUP_EPSILON = 0.00064
F32 = jnp.float32
BF16 = jnp.bfloat16
MESH = pl.DeviceIdType.MESH


def nn(a, b):
    return jnp.dot(a, b, preferred_element_type=F32)


def nt(a, b):
    return lax.dot_general(a, b, (((1,), (1,)), ((), ())), preferred_element_type=F32)


def parts(a, count):
    out = []
    for k in range(count):
        piece = a.astype(BF16)
        out.append(piece)
        if k < count - 1:
            a = a - piece.astype(F32)
    return out


def mm(a, b, product=nn, na=2, nb=2):
    pa = [a] if a.dtype == BF16 else parts(a, na)
    pb = [b] if b.dtype == BF16 else parts(b, nb)
    total = None
    for i, x in enumerate(pa):
        for j, y in enumerate(pb):
            if i + j < max(len(pa), len(pb)):
                term = product(x, y)
                total = term if total is None else total + term
    return total


def square(a, b):
    (ah, al), (bh, bl) = parts(a, 2), parts(b, 2)
    both = nn(
        jnp.concatenate([ah, al], axis=1),
        jnp.concatenate(
            [
                jnp.concatenate([bh, bl], axis=1),
                jnp.concatenate([bh, jnp.zeros_like(bl)], axis=1),
            ],
            axis=0,
        ),
    )
    return both[:, :L] + both[:, L:]


def iota(shape, dim):
    return lax.broadcasted_iota(jnp.int32, shape, dim)


def sigmoid(v):
    return 1.0 / (1.0 + jnp.exp(-v))


def column(row):
    n = row.shape[1]
    return jnp.sum(
        jnp.where(iota((n, n), 0) == iota((n, n), 1), row, 0.0), axis=1, keepdims=True
    )


def beside_identity(f):
    top = jnp.where(iota((HC, 2 * HC), 0) == iota((HC, 2 * HC), 1), 1.0, 0.0)
    return jnp.concatenate([top.astype(f.dtype), f], axis=0)


def joined(late, early):
    return mm(late, beside_identity(early))


def solved(right, n):
    r, c = iota((L, L), 0), iota((L, L), 1)
    eye = jnp.where(r == c, 1.0, 0.0)
    same8 = r // 8 == c // 8
    same32 = r // 32 == c // 32
    small = jnp.where(same8, n, 0.0)
    middle = jnp.where(same32 & (r // 8 != c // 8), n, 0.0)
    large = jnp.where(same32, 0.0, n)
    two = square(small, small)
    four = square(two, two)
    first = eye + small + two + square(small, two)
    x = first + square(first, four)
    step = square(middle, x)
    x = x + square(x, step)
    x = x + square(x, square(step, step))
    step = square(large, x)
    y = square(right, x)
    y = y + square(y, step)
    return y + square(y, square(step, step))


def local_block(rec, key, val, removal, lr, ld):
    s, t = iota((L, L), 0), iota((L, L), 1)
    upto = jnp.where(s <= t, 1.0, 0.0).astype(BF16)
    cum = sum(nn(p, upto) for p in parts(ld, 3))
    ref, end = cum[:, L // 2 - 1 : L // 2], cum[:, L - 1 : L]
    eq = jnp.exp(cum - ref)
    eb = jnp.exp(cum - ld - ref)
    ek = jnp.exp(ref - cum)
    eref, eend = jnp.exp(ref), jnp.exp(end - ref)
    qn, qr = -removal * eb, rec * eq
    kb, kk = removal * lr * ek, key * lr * ek
    keys = jnp.concatenate([kb.T, kk.T], axis=0)
    both = mm(keys, jnp.concatenate([qn, qr], axis=1))
    lb = jnp.where(s < t, both[:L, :L], 0.0)
    ob = jnp.where(s <= t, both[:L, L:], 0.0)
    lk = jnp.where(s < t, both[L:, :L], 0.0)
    ok = jnp.where(s <= t, both[L:, L:], 0.0)
    return lb, ob, lk, ok, kb, kk, qn, qr, eref, eend, jnp.exp(end), val


def local_result(lb, ob, lk, ok, kb, kk, qn, qr, eref, eend, whole, val):
    valued = mm(val, jnp.concatenate([lk, ok], axis=1))
    right = jnp.concatenate([valued[:, :L], qn * eref], axis=0)
    corr = solved(right, lb)
    z = square(corr, ob) + jnp.concatenate([valued[:, L:], qr * eref], axis=0)
    aug = jnp.concatenate([val, jnp.zeros_like(val)], axis=0)
    f = mm(
        jnp.concatenate([kb * eend, kk * eend], axis=1),
        jnp.concatenate([corr, aug.astype(F32)], axis=1),
        nt,
    )
    f = f + jnp.where(
        iota((HC, 2 * HC), 0) + HC == iota((HC, 2 * HC), 1), whole, 0.0
    )
    return f, z


def kernel(nx, nz, *refs):
    from_hbm = refs[:21]
    out_a, out_b = refs[21:23]
    (exr, eng, idx, cgu, cd, rec, key, val, dec, lrn, spk, dco, gat, hng, wts, rg, ru, rd, how, png, nb, dout, darr, ep, epr, es, rb, rout, rarr,
     sp, spr, ss, sb, ho, ap, apr, aps, ab, xarr, zs, zarr, load, pair_s, pair_r, dsend, drecv,
     ysend, yrecv, rsend, rrecv, xsend, xrecv, zsend, zrecv) = refs[23:]
    n_ep = nx * nz
    tb = exr.shape[0]
    rows = n_ep * CAP
    slots = rows * GROUPS
    me, t = lax.axis_index("ep"), lax.axis_index("tp")
    y, c = lax.div(t, 2), lax.rem(t, 2)
    z, x = lax.div(me, nx), lax.rem(me, nx)
    other = t + 1 - 2 * c

    def remote(src, dst, send, recv, where):
        return pltpu.make_async_remote_copy(
            src_ref=src, dst_ref=dst, send_sem=send, recv_sem=recv,
            device_id=where, device_id_type=MESH,
        )

    def drain(ref, sem):
        pltpu.make_async_copy(ref, ref, sem).wait()

    targets = (
        exr, eng, idx, cgu.at[0:HC], cgu.at[HC : 2 * HC], cd, rec, key, val, dec, lrn, spk, dco,
        gat, hng, wts, rg, ru, rd, how, png,
    )
    loads = [
        pltpu.make_async_copy(a, b, load.at[k])
        for k, (a, b) in enumerate(zip(from_hbm, targets, strict=True))
    ]
    for copy in loads:
        copy.start()

    def ready(start, stop):
        for copy in loads[start:stop]:
            copy.wait()

    unit = jnp.where(iota((HC, 2 * HC), 0) + HC == iota((HC, 2 * HC), 1), 1.0, 0.0)
    for k in range(nz):
        zarr[k] = unit.astype(BF16)

    barrier = pltpu.get_barrier_semaphore()
    pl.semaphore_signal(barrier, inc=1, device_id={"tp": other}, device_id_type=MESH)
    for d in range(1, GROUPS):
        pl.semaphore_signal(
            barrier, inc=1, device_id={"tp": 2 * lax.rem(y + d, GROUPS) + c}, device_id_type=MESH
        )

    def greet(d, carry):
        pl.semaphore_signal(
            barrier, inc=1, device_id={"ep": lax.rem(me + d, n_ep)}, device_id_type=MESH
        )
        return carry

    lax.fori_loop(1, n_ep, greet, 0)

    ready(0, 3)
    wide = exr[...].astype(F32)
    scale = lax.rsqrt(jnp.mean(wide * wide, axis=1, keepdims=True) + NORM_EPSILON)
    nb[...] = (wide * scale * eng[...]).astype(BF16)

    width = darr.shape[2]
    first, second = idx[0:1, :], idx[1:2, :]
    i = iota((slots, tb), 0)
    expert = lax.div(i, 16) * GROUPS + y
    hits = jnp.where((first == expert) | (second == expert), 1.0, 0.0)
    earlier = jnp.where(iota((tb, tb), 0) < iota((tb, tb), 1), 1.0, 0.0).astype(BF16)
    rank = nn(hits.astype(BF16), earlier)
    mine = jnp.where(rank == lax.rem(lax.div(i, 8), 2).astype(F32), hits, 0.0)
    piece = lax.rem(i, 8)
    picks = jnp.concatenate(
        [jnp.where(piece == j, mine, 0.0).astype(BF16) for j in range(GROUPS)], axis=1
    )
    stacked = jnp.concatenate(
        [
            nb[:, pl.ds(pl.multiple_of((c * GROUPS + j) * width, width), width)]
            for j in range(GROUPS)
        ],
        axis=0,
    )
    dout[...] = nn(picks, stacked).astype(BF16)
    own = pl.ds(pl.multiple_of(me * 16, 16), 16)
    darr[c, own, :] = dout[own, :]

    ready(3, 6)
    gate_up = nt(cgu[...], nb[...])
    g, u = gate_up[:HC], gate_up[HC:]
    hidden = (g * sigmoid(g) * u).T.astype(BF16)
    shared = nn(hidden, cd[...]).astype(BF16)
    cols = shared.shape[1] // (2 * GROUPS)
    for k in range(2 * GROUPS):
        sp[k % 2, k // 2] = shared[:, k * cols : (k + 1) * cols]

    ready(6, 13)
    k_in = key[...].astype(F32)
    pre = column(dco[...]) + jnp.tanh(dec[...].astype(F32))
    ld = spk[...] - sigmoid(pre) * math.exp(-0.5)
    lr = sigmoid(lrn[...].astype(F32))
    removal = k_in * lax.rsqrt(jnp.sum(k_in * k_in, axis=0, keepdims=True) + NORM_EPSILON)
    r_in = rec[...].astype(F32)
    prepared = []
    for b in range(key.shape[1] // L):
        at = slice(b * L, (b + 1) * L)
        prepared.append(
            local_block(r_in[:, at], k_in[:, at], val[:, at], removal[:, at], lr[:, at], ld[:, at])
        )

    pl.semaphore_wait(barrier, GROUPS + n_ep - 1)

    def send_rows(d, carry):
        to = lax.rem(me + d, n_ep)
        remote(
            dout.at[pl.ds(pl.multiple_of(to * 16, 16), 16)], darr.at[c, own],
            dsend, drecv, {"ep": to},
        ).start()
        return carry

    lax.fori_loop(1, n_ep, send_rows, 0)
    pair_shared = remote(sp.at[1 - c], spr, pair_s.at[0], pair_r.at[0], {"tp": other})
    pair_shared.start()

    blocks = [local_result(*values) for values in prepared]
    f, z_out = blocks[0]
    z_all = [z_out]
    for later_f, later_z in blocks[1:]:
        z_all.append(mm(beside_identity(f).T, later_z))
        f = joined(later_f, f)
    z_all = jnp.concatenate(z_all, axis=1)
    xarr[x] = f.astype(BF16)

    x_sends = [
        remote(
            xarr.at[x], xarr.at[x], xsend.at[d - 1], xrecv.at[d - 1],
            {"ep": z * nx + lax.rem(x + d, nx)},
        )
        for d in range(1, nx)
    ]
    for copy in x_sends:
        copy.start()

    pair_shared.wait()
    ss[...] = (sp[c].astype(F32) + spr[...].astype(F32)).astype(BF16)
    sb[y] = ss[y]
    y_sends = []
    for k, d in enumerate(FAR_FIRST):
        to = lax.rem(y + d, GROUPS)
        y_sends.append(
            remote(ss.at[to], sb.at[y], ysend.at[0, k], yrecv.at[0, k], {"tp": 2 * to + c})
        )
        y_sends[-1].start()

    for copy in x_sends:
        copy.wait()
    stretch = [xarr[k] for k in range(nx)]
    before = unit
    total = stretch[0]
    for k in range(1, nx):
        before = jnp.where(x == k, total.astype(F32), before)
        total = joined(stretch[k], total)
    zs[...] = total.astype(BF16)
    for d in range(1, nz):
        @pl.when(z + d < nz)
        def _():
            remote(
                zs, zarr.at[z], zsend.at[d - 1], zrecv.at[z], {"ep": (z + d) * nx + x}
            ).start()

    z_all = mm(beside_identity(before).T, z_all)

    ready(13, 16)
    q = iota((slots, slots), 1)
    r = iota((slots, slots), 0)
    source = lax.div(lax.rem(r, 16), 2) * rows + lax.rem(r, 2) * n_ep + lax.div(r, 16)
    back = jnp.where(q == source, 1.0, 0.0).astype(BF16)
    lines = jnp.concatenate(
        [first.astype(F32), second.astype(F32), wts[...], jnp.zeros((4, tb), F32)], axis=0
    ).T
    q = iota((tb, slots), 1)
    expert = (lax.div(q, 16) * GROUPS + lax.div(lax.rem(q, 16), 2)).astype(F32)
    hit_a = jnp.where(lines[:, 0:1] == expert, 1.0, 0.0)
    hit_b = jnp.where(lines[:, 1:2] == expert, 1.0, 0.0)
    earlier = jnp.where(iota((tb, tb), 0) > iota((tb, tb), 1), 1.0, 0.0).astype(BF16)
    rank = nn(earlier, (hit_a + hit_b).astype(BF16))
    weight = jnp.where(
        rank == lax.rem(q, 2).astype(F32), hit_a * lines[:, 2:3] + hit_b * lines[:, 3:4], 0.0
    )

    r, q = iota((slots, slots), 0), iota((slots, slots), 1)
    source = lax.rem(r, n_ep) * 16 + lax.rem(lax.div(r, n_ep), 2) * 8 + lax.div(r, rows)
    turn = jnp.where(q == source, 1.0, 0.0).astype(BF16)
    drain(darr.at[c, 0 : (n_ep - 1) * 16], drecv)
    pair_rows = remote(darr.at[c], darr.at[c], pair_s.at[4], pair_r.at[4], {"tp": other})
    pair_rows.start()
    pair_rows.wait()

    turned = nn(turn, jnp.concatenate([darr[0], darr[1]], axis=1)).astype(BF16)
    rows_in = jnp.concatenate(
        [
            turned[j * rows : (j + 1) * rows, h * width : (h + 1) * width]
            for h in range(2)
            for j in range(GROUPS)
        ],
        axis=1,
    )
    ready(16, 18)
    g, u = nn(rows_in, rg[...]), nn(rows_in, ru[...])
    hidden = (g * sigmoid(g) * u).astype(BF16)
    ready(18, 19)
    routed = nn(hidden, rd[...]).astype(BF16)
    for k in range(2 * GROUPS):
        ep[k % 2, k // 2] = routed[:, k * cols : (k + 1) * cols]
    pair_routed = remote(ep.at[1 - c], epr, pair_s.at[1], pair_r.at[1], {"tp": other})
    pair_routed.start()

    pair_routed.wait()
    es[...] = (ep[c].astype(F32) + epr[...].astype(F32)).astype(BF16)
    rb[y] = es[y]
    for k, d in enumerate(FAR_FIRST):
        to = lax.rem(y + d, GROUPS)
        y_sends.append(
            remote(es.at[to], rb.at[y], ysend.at[1, k], yrecv.at[1, k], {"tp": 2 * to + c})
        )
        y_sends[-1].start()

    for k in range(nz - 1):
        @pl.when(k < z)
        def _():
            drain(zarr.at[k], zrecv.at[k])

    level = [zarr[k] for k in range(nz - 1)] if nz > 1 else [unit.astype(BF16)]
    while len(level) > 1:
        nxt = [joined(level[k + 1], level[k]) for k in range(0, len(level) - 1, 2)]
        if len(level) % 2:
            nxt.append(level[-1].astype(F32))
        level = nxt

    carried = level[0].astype(F32)
    head = mm(beside_identity(carried).T[:HC], z_all)
    centred = head - jnp.mean(head, axis=0, keepdims=True)
    normed = centred * lax.rsqrt(jnp.mean(centred * centred, axis=0, keepdims=True) + GROUP_EPSILON)
    heads_out = normed * column(hng[...]) * sigmoid(gat[...].astype(F32))
    heads_out = heads_out.T.astype(BF16)
    own_rows = out_a.shape[0]
    ho[...] = heads_out.reshape(GROUPS, 2, own_rows, HC)
    ready(19, 20)

    order = FAR_FIRST + (0,)
    half = GROUPS // 2

    def product(first, core):
        lines = [ho[lax.rem(y + d, GROUPS), core] for d in order[first : first + half]]
        return nn(jnp.concatenate(lines, axis=0), how[...])

    pair_mix = []
    for k in range(2):
        at = slice(k * half, (k + 1) * half)
        ap[at] = product(k * half, 1 - c).astype(BF16).reshape(half, own_rows, -1)
        pair_mix.append(
            remote(ap.at[at], apr.at[at], pair_s.at[2 + k], pair_r.at[2 + k], {"tp": other})
        )
        pair_mix[-1].start()
    mixed = [product(k * half, c).astype(BF16).astype(F32) for k in range(2)]

    a_sends = []
    for k in range(2):
        at = slice(k * half, (k + 1) * half)
        pair_mix[k].wait()
        aps[at] = (mixed[k].reshape(half, own_rows, -1) + apr[at].astype(F32)).astype(BF16)
        for j in range(k * half, (k + 1) * half):
            if order[j]:
                to = lax.rem(y + order[j], GROUPS)
                a_sends.append(
                    remote(
                        aps.at[j], ab.at[y], ysend.at[2, j], yrecv.at[2, j], {"tp": 2 * to + c}
                    )
                )
                a_sends[-1].start()
    ab[y] = aps[GROUPS - 1]

    for copy in y_sends[GROUPS - 1 :]:
        copy.wait()
    every = jnp.concatenate([rb[k] for k in range(GROUPS)], axis=0)
    rout[...] = nn(back, every).astype(BF16)
    rarr[own, :] = rout[own, :]

    def send_back(d, carry):
        to = lax.rem(me + d, n_ep)
        remote(
            rout.at[pl.ds(pl.multiple_of(to * 16, 16), 16)], rarr.at[own],
            rsend, rrecv, {"ep": to},
        ).start()
        return carry

    lax.fori_loop(1, n_ep, send_back, 0)

    for copy in y_sends[: GROUPS - 1]:
        copy.wait()
    drain(rarr.at[0 : (n_ep - 1) * 16], rrecv)
    answer = mm(weight, rarr[...])
    for k in range(GROUPS):
        answer = answer + sb[k].astype(F32)
    out_b[...] = answer.astype(BF16)

    ready(20, 21)
    for copy in a_sends:
        copy.wait()
    mix = ab[0].astype(F32)
    for k in range(1, GROUPS):
        mix = mix + ab[k].astype(F32)
    scale = lax.rsqrt(jnp.mean(mix * mix, axis=1, keepdims=True) + NORM_EPSILON)
    out_a[...] = (mix * scale * png[...]).astype(BF16)

    for d in range(1, nz):
        @pl.when(z + d < nz)
        def _():
            drain(zs, zsend.at[d - 1])
    drain(dout.at[0 : (n_ep - 1) * 16], dsend)
    drain(rout.at[0 : (n_ep - 1) * 16], rsend)


def solution(mesh):
    n_ep = mesh.shape["ep"]
    nx = 4 if n_ep % 4 == 0 else n_ep
    nz = n_ep // nx

    def body(rec, key, val, dec, lrn, gat, dco, spk, hng, how, png, exr, eng, idx, wts,
             rg, ru, rd, cg, cu, cd):
        ta, d = rec.shape[0], how.shape[1]
        tb = exr.shape[0]
        own, cols = ta // (2 * GROUPS), d // (2 * GROUPS)
        rows = n_ep * CAP
        width = d // (2 * GROUPS)
        line = lambda a: a.reshape(1, -1)
        given = [
            exr, line(eng), idx.T, cg.T, cu.T, cd, rec.T, key.T, val.T, dec.T, lrn.T, spk.T,
            line(dco), gat.T, line(hng), wts.T, rg[0], ru[0], rd[0], how, line(png),
        ]
        held = [pltpu.VMEM(a.shape, a.dtype) for a in given]
        held[3:5] = [pltpu.VMEM((2 * HC, d), BF16)]
        vmem = pl.BlockSpec(memory_space=pltpu.VMEM)
        dma = pltpu.SemaphoreType.DMA
        return pl.pallas_call(
            functools.partial(kernel, nx, nz),
            out_shape=(
                jax.ShapeDtypeStruct((own, d), BF16),
                jax.ShapeDtypeStruct((tb, cols), BF16),
            ),
            in_specs=[pl.BlockSpec(memory_space=pltpu.HBM)] * len(given),
            out_specs=(vmem, vmem),
            scratch_shapes=[
                *held,
                pltpu.VMEM((tb, d), BF16),
                pltpu.VMEM((n_ep * 16, width), BF16),
                pltpu.VMEM((2, n_ep * 16, width), BF16),
                pltpu.VMEM((2, GROUPS, rows, cols), BF16),
                pltpu.VMEM((GROUPS, rows, cols), BF16),
                pltpu.VMEM((GROUPS, rows, cols), BF16),
                pltpu.VMEM((GROUPS, rows, cols), BF16),
                pltpu.VMEM((n_ep * 16, cols), BF16),
                pltpu.VMEM((n_ep * 16, cols), BF16),
                pltpu.VMEM((2, GROUPS, tb, cols), BF16),
                pltpu.VMEM((GROUPS, tb, cols), BF16),
                pltpu.VMEM((GROUPS, tb, cols), BF16),
                pltpu.VMEM((GROUPS, tb, cols), BF16),
                pltpu.VMEM((GROUPS, 2, own, HC), BF16),
                pltpu.VMEM((GROUPS, own, d), BF16),
                pltpu.VMEM((GROUPS, own, d), BF16),
                pltpu.VMEM((GROUPS, own, d), BF16),
                pltpu.VMEM((GROUPS, own, d), BF16),
                pltpu.VMEM((nx, HC, 2 * HC), BF16),
                pltpu.VMEM((HC, 2 * HC), BF16),
                pltpu.VMEM((nz, HC, 2 * HC), BF16),
                dma((len(given),)),
                dma((5,)),
                dma((5,)),
                dma,
                dma,
                dma((3, GROUPS - 1)),
                dma((3, GROUPS - 1)),
                dma,
                dma,
                dma((max(nx - 1, 1),)),
                dma((max(nx - 1, 1),)),
                dma((max(nz - 1, 1),)),
                dma((max(nz, 1),)),
            ],
            compiler_params=pltpu.CompilerParams(
                collective_id=0, has_side_effects=True, vmem_limit_bytes=67_043_328
            ),
        )(*given)

    placed = (
        P("ep", "tp"), P("ep", "tp"), P("ep", "tp"), P("ep", "tp"), P("ep", "tp"), P("ep", "tp"),
        P("tp"), P("ep", "tp"), P("tp"), P("tp", None), P(), P("ep", None), P(), P("ep", None),
        P("ep", None), P(("ep", "tp"), None, None), P(("ep", "tp"), None, None),
        P(("ep", "tp"), None, None), P(None, "tp"), P(None, "tp"), P("tp", None),
    )
    return jax.shard_map(
        body,
        mesh=mesh,
        in_specs=placed,
        out_specs=(P(("ep", "tp"), None), P("ep", "tp")),
        check_vma=False,
    )
```

```python
import functools
import math

import jax
import jax.numpy as jnp
from jax import lax
from jax.experimental import pallas as pl
from jax.experimental.pallas import tpu as pltpu
from jax.sharding import PartitionSpec as P

HC = 64
L = 128
GROUPS = 8
CAP = 2
FAR_FIRST = (4, 3, 5, 2, 6, 1, 7)
NORM_EPSILON = 1e-06
GROUP_EPSILON = 0.00064
F32 = jnp.float32
BF16 = jnp.bfloat16
MESH = pl.DeviceIdType.MESH


def nn(a, b):
    return jnp.dot(a, b, preferred_element_type=F32)


def nt(a, b):
    return lax.dot_general(a, b, (((1,), (1,)), ((), ())), preferred_element_type=F32)


def parts(a, count):
    out = []
    for k in range(count):
        piece = a.astype(BF16)
        out.append(piece)
        if k < count - 1:
            a = a - piece.astype(F32)
    return out


def mm(a, b, product=nn, na=2, nb=2):
    pa = [a] if a.dtype == BF16 else parts(a, na)
    pb = [b] if b.dtype == BF16 else parts(b, nb)
    total = None
    for i, x in enumerate(pa):
        for j, y in enumerate(pb):
            if i + j < max(len(pa), len(pb)):
                term = product(x, y)
                total = term if total is None else total + term
    return total


def square(a, b):
    (ah, al), (bh, bl) = parts(a, 2), parts(b, 2)
    both = nn(
        jnp.concatenate([ah, al], axis=1),
        jnp.concatenate(
            [
                jnp.concatenate([bh, bl], axis=1),
                jnp.concatenate([bh, jnp.zeros_like(bl)], axis=1),
            ],
            axis=0,
        ),
    )
    return both[:, :L] + both[:, L:]


def iota(shape, dim):
    return lax.broadcasted_iota(jnp.int32, shape, dim)


def sigmoid(v):
    return 1.0 / (1.0 + jnp.exp(-v))


def column(row):
    n = row.shape[1]
    return jnp.sum(
        jnp.where(iota((n, n), 0) == iota((n, n), 1), row, 0.0), axis=1, keepdims=True
    )


def beside_identity(f):
    top = jnp.where(iota((HC, 2 * HC), 0) == iota((HC, 2 * HC), 1), 1.0, 0.0)
    return jnp.concatenate([top.astype(f.dtype), f], axis=0)


def joined(late, early):
    return mm(late, beside_identity(early))


def solved(right, n):
    r, c = iota((L, L), 0), iota((L, L), 1)
    eye = jnp.where(r == c, 1.0, 0.0)
    same8 = r // 8 == c // 8
    same32 = r // 32 == c // 32
    small = jnp.where(same8, n, 0.0)
    middle = jnp.where(same32 & (r // 8 != c // 8), n, 0.0)
    large = jnp.where(same32, 0.0, n)
    two = square(small, small)
    four = square(two, two)
    first = eye + small + two + square(small, two)
    x = first + square(first, four)
    step = square(middle, x)
    x = x + square(x, step)
    x = x + square(x, square(step, step))
    step = square(large, x)
    y = square(right, x)
    y = y + square(y, step)
    return y + square(y, square(step, step))


def local_block(rec, key, val, removal, lr, ld):
    s, t = iota((L, L), 0), iota((L, L), 1)
    upto = jnp.where(s <= t, 1.0, 0.0).astype(BF16)
    cum = sum(nn(p, upto) for p in parts(ld, 3))
    ref, end = cum[:, L // 2 - 1 : L // 2], cum[:, L - 1 : L]
    eq = jnp.exp(cum - ref)
    eb = jnp.exp(cum - ld - ref)
    ek = jnp.exp(ref - cum)
    eref, eend = jnp.exp(ref), jnp.exp(end - ref)
    qn, qr = -removal * eb, rec * eq
    kb, kk = removal * lr * ek, key * lr * ek
    keys = jnp.concatenate([kb.T, kk.T], axis=0)
    both = mm(keys, jnp.concatenate([qn, qr], axis=1))
    lb = jnp.where(s < t, both[:L, :L], 0.0)
    ob = jnp.where(s <= t, both[:L, L:], 0.0)
    lk = jnp.where(s < t, both[L:, :L], 0.0)
    ok = jnp.where(s <= t, both[L:, L:], 0.0)
    return lb, ob, lk, ok, kb, kk, qn, qr, eref, eend, jnp.exp(end), val


def local_result(lb, ob, lk, ok, kb, kk, qn, qr, eref, eend, whole, val):
    valued = mm(val, jnp.concatenate([lk, ok], axis=1))
    right = jnp.concatenate([valued[:, :L], qn * eref], axis=0)
    corr = solved(right, lb)
    z = square(corr, ob) + jnp.concatenate([valued[:, L:], qr * eref], axis=0)
    aug = jnp.concatenate([val, jnp.zeros_like(val)], axis=0)
    f = mm(
        jnp.concatenate([kb * eend, kk * eend], axis=1),
        jnp.concatenate([corr, aug.astype(F32)], axis=1),
        nt,
    )
    f = f + jnp.where(
        iota((HC, 2 * HC), 0) + HC == iota((HC, 2 * HC), 1), whole, 0.0
    )
    return f, z


def kernel(nx, nz, *refs):
    from_hbm = refs[:21]
    out_a, out_b = refs[21:23]
    (exr, eng, idx, cgu, cd, rec, key, val, dec, lrn, spk, dco, gat, hng, wts, rg, ru, rd, how, png, nb, dout, darr, ep, epr, es, rb, rout, rarr,
     sp, spr, ss, sb, ho, ap, apr, aps, ring_in, xarr, zs, zarr, load, pair_s, pair_r, dsend, drecv,
     ysend, yrecv, rsum_s, rsum_r, rsend, rrecv, xsend, xrecv, zsend, zrecv, zsc) = refs[23:]
    n_ep = nx * nz
    tb = exr.shape[0]
    rows = n_ep * CAP
    slots = rows * GROUPS
    me, t = lax.axis_index("ep"), lax.axis_index("tp")
    y, c = lax.div(t, 2), lax.rem(t, 2)
    z, x = lax.div(me, nx), lax.rem(me, nx)
    other = t + 1 - 2 * c

    def remote(src, dst, send, recv, where):
        return pltpu.make_async_remote_copy(
            src_ref=src, dst_ref=dst, send_sem=send, recv_sem=recv,
            device_id=where, device_id_type=MESH,
        )

    def drain(ref, sem):
        pltpu.make_async_copy(ref, ref, sem).wait()

    def ready(start, stop):
        for copy in loads[start:stop]:
            copy.wait()

    targets = (
        exr, eng, idx, cgu.at[0:HC], cgu.at[HC : 2 * HC], cd, rec, key, val, dec, lrn, spk, dco,
        gat, hng, wts, rg, ru, rd, how, png,
    )
    loads = [
        pltpu.make_async_copy(a, b, load.at[k])
        for k, (a, b) in enumerate(zip(from_hbm, targets, strict=True))
    ]
    for copy in loads[:3]:
        copy.start()

    unit = jnp.where(iota((HC, 2 * HC), 0) + HC == iota((HC, 2 * HC), 1), 1.0, 0.0)
    for k in range(nz):
        zarr[k] = unit.astype(BF16)

    barrier = pltpu.get_barrier_semaphore()

    def greet(where):
        pl.semaphore_signal(barrier, inc=1, device_id=where, device_id_type=MESH)

    def greet_ep(d, carry):
        greet({"ep": lax.rem(me + d, n_ep)})
        return carry

    lax.fori_loop(n_ep // 2, n_ep, greet_ep, 0)
    lax.fori_loop(1, n_ep // 2, greet_ep, 0)
    for d in FAR_FIRST:
        greet({"tp": 2 * lax.rem(y + d, GROUPS) + c})
    greet({"tp": other})

    for k in (*range(6, 13), *range(3, 6), *range(16, 20), *range(13, 16), 20):
        loads[k].start()
    ready(2, 3)
    width = darr.shape[2]
    first, second = idx[0:1, :], idx[1:2, :]
    i = iota((slots, tb), 0)
    expert = lax.div(i, 16) * GROUPS + y
    hits = jnp.where((first == expert) | (second == expert), 1.0, 0.0)
    earlier = jnp.where(iota((tb, tb), 0) < iota((tb, tb), 1), 1.0, 0.0).astype(BF16)
    rank = nn(hits.astype(BF16), earlier)
    mine = jnp.where(rank == lax.rem(lax.div(i, 8), 2).astype(F32), hits, 0.0)
    piece = lax.rem(i, 8)
    picks = jnp.concatenate(
        [jnp.where(piece == j, mine, 0.0).astype(BF16) for j in range(GROUPS)], axis=1
    )

    ready(0, 2)
    wide = exr[...].astype(F32)
    scale = lax.rsqrt(jnp.mean(wide * wide, axis=1, keepdims=True) + NORM_EPSILON)
    nb[...] = (wide * scale * eng[...]).astype(BF16)

    stacked = jnp.concatenate(
        [
            nb[:, pl.ds(pl.multiple_of((c * GROUPS + j) * width, width), width)]
            for j in range(GROUPS)
        ],
        axis=0,
    )
    dout[...] = nn(picks, stacked).astype(BF16)
    own = pl.ds(pl.multiple_of(me * 16, 16), 16)
    darr[c, own, :] = dout[own, :]

    def to_all(src, dst, send, recv, groups):
        for zo in groups:
            for xo in sorted(range(nx), key=lambda v: -min(v, nx - v)):
                if zo or xo:
                    to = lax.rem(z + zo, nz) * nx + lax.rem(x + xo, nx)
                    remote(
                        src.at[pl.ds(pl.multiple_of(to * 16, 16), 16)], dst, send, recv, {"ep": to}
                    ).start()

    far_z = sorted(range(1, nz), key=lambda v: -min(v, nz - v))

    def meet():
        pl.semaphore_wait(barrier, GROUPS + n_ep - 1)
        to_all(dout, darr.at[c, own], dsend, drecv, (*far_z, 0))

    @pl.when(z >= nz // 2)
    def _():
        meet()

    ready(6, 13)
    k_in = key[...].astype(F32)
    pre = column(dco[...]) + jnp.tanh(dec[...].astype(F32))
    ld = spk[...] - sigmoid(pre) * math.exp(-0.5)
    lr = sigmoid(lrn[...].astype(F32))
    removal = k_in * lax.rsqrt(jnp.sum(k_in * k_in, axis=0, keepdims=True) + NORM_EPSILON)
    r_in = rec[...].astype(F32)
    prepared = []
    for b in range(key.shape[1] // L):
        at = slice(b * L, (b + 1) * L)
        prepared.append(
            local_block(r_in[:, at], k_in[:, at], val[:, at], removal[:, at], lr[:, at], ld[:, at])
        )

    ready(3, 6)
    gate_up = nt(cgu[...], nb[...])
    g, u = gate_up[:HC], gate_up[HC:]
    hidden = (g * sigmoid(g) * u).T.astype(BF16)
    shared = nn(hidden, cd[...]).astype(BF16)
    cols = shared.shape[1] // (2 * GROUPS)
    for k in range(2 * GROUPS):
        sp[k % 2, k // 2] = shared[:, k * cols : (k + 1) * cols]

    blocks = [local_result(*values) for values in prepared]
    f, z_out = blocks[0]
    z_all = [z_out]
    for later_f, later_z in blocks[1:]:
        z_all.append(mm(beside_identity(f).T, later_z))
        f = joined(later_f, f)
    z_all = jnp.concatenate(z_all, axis=1)
    xarr[x] = f.astype(BF16)

    @pl.when(z < nz // 2)
    def _():
        meet()

    x_sends = [
        remote(
            xarr.at[x], xarr.at[x], xsend.at[d - 1], xrecv.at[d - 1],
            {"ep": z * nx + lax.rem(x + d, nx)},
        )
        for d in range(1, nx)
    ]
    for copy in x_sends:
        copy.start()

    pair_shared = remote(sp.at[1 - c], spr, pair_s.at[0], pair_r.at[0], {"tp": other})
    pair_shared.start()

    ready(13, 16)
    q = iota((slots, slots), 1)
    r = iota((slots, slots), 0)
    source = lax.div(lax.rem(r, 16), 2) * rows + lax.rem(r, 2) * n_ep + lax.div(r, 16)
    back = jnp.where(q == source, 1.0, 0.0).astype(BF16)
    lines = jnp.concatenate(
        [first.astype(F32), second.astype(F32), wts[...], jnp.zeros((4, tb), F32)], axis=0
    ).T
    q = iota((tb, slots), 1)
    expert = (lax.div(q, 16) * GROUPS + lax.div(lax.rem(q, 16), 2)).astype(F32)
    hit_a = jnp.where(lines[:, 0:1] == expert, 1.0, 0.0)
    hit_b = jnp.where(lines[:, 1:2] == expert, 1.0, 0.0)
    earlier = jnp.where(iota((tb, tb), 0) > iota((tb, tb), 1), 1.0, 0.0).astype(BF16)
    rank = nn(earlier, (hit_a + hit_b).astype(BF16))
    weight = jnp.where(
        rank == lax.rem(q, 2).astype(F32), hit_a * lines[:, 2:3] + hit_b * lines[:, 3:4], 0.0
    )

    pair_shared.wait()
    ss[...] = (sp[c].astype(F32) + spr[...].astype(F32)).astype(BF16)
    sb[y] = ss[y]
    y_sends = []
    for k, d in enumerate(FAR_FIRST):
        to = lax.rem(y + d, GROUPS)
        y_sends.append(
            remote(ss.at[to], sb.at[y], ysend.at[0, k], yrecv.at[0, k], {"tp": 2 * to + c})
        )
        y_sends[-1].start()

    for copy in x_sends:
        copy.wait()
    stretch = [xarr[k] for k in range(nx)]
    before = unit
    total = stretch[0]
    for k in range(1, nx):
        before = jnp.where(x == k, total.astype(F32), before)
        total = joined(stretch[k], total)
    zs[...] = total.astype(BF16)
    for d in range(1, nz):
        @pl.when(z + d < nz)
        def _():
            remote(
                zs, zarr.at[z], zsend.at[d - 1], zrecv.at[z], {"ep": (z + d) * nx + x}
            ).start()

    zsc[...] = mm(beside_identity(before).T, z_all)

    order = FAR_FIRST + (0,)

    def ring(step, way):
        k = 3 * way + step
        to = lax.rem(y + (GROUPS - 1 if way else 1), GROUPS)
        slot = order.index(4 + step if way else 3 - step)
        return remote(aps.at[slot], ring_in.at[k], rsum_s.at[k], rsum_r.at[k], {"tp": 2 * to + c})

    def ring_on(step):
        for way in range(2):
            if step < 3 + way:
                ring(step - 1, way).wait_recv()
                slot = order.index(4 + step if way else 3 - step)
                arrived = ring_in[3 * way + step - 1].astype(F32)
                aps[slot] = (aps[slot].astype(F32) + arrived).astype(BF16)
                ring(step, way).start()

    def project_heads():
        for k in range(nz - 1):
            @pl.when(k < z)
            def _():
                drain(zarr.at[k], zrecv.at[k])

        level = [zarr[k] for k in range(nz - 1)] if nz > 1 else [unit.astype(BF16)]
        while len(level) > 1:
            nxt = [joined(level[k + 1], level[k]) for k in range(0, len(level) - 1, 2)]
            if len(level) % 2:
                nxt.append(level[-1].astype(F32))
            level = nxt

        carried = level[0].astype(F32)
        head = mm(beside_identity(carried).T[:HC], zsc[...])
        centred = head - jnp.mean(head, axis=0, keepdims=True)
        normed = centred * lax.rsqrt(jnp.mean(centred * centred, axis=0, keepdims=True) + GROUP_EPSILON)
        heads_out = normed * column(hng[...]) * sigmoid(gat[...].astype(F32))
        heads_out = heads_out.T.astype(BF16)
        own_rows = out_a.shape[0]
        ho[...] = heads_out.reshape(GROUPS, 2, own_rows, HC)
        ready(19, 20)

        half = GROUPS // 2

        def product(first, core):
            lines = [ho[lax.rem(y + d, GROUPS), core] for d in order[first : first + half]]
            return nn(jnp.concatenate(lines, axis=0), how[...])

        pair_mix = []
        for k in range(2):
            at = slice(k * half, (k + 1) * half)
            ap[at] = product(k * half, 1 - c).astype(BF16).reshape(half, own_rows, -1)
            pair_mix.append(
                remote(ap.at[at], apr.at[at], pair_s.at[2 + k], pair_r.at[2 + k], {"tp": other})
            )
            pair_mix[-1].start()
        mixed = [product(k * half, c).astype(BF16).astype(F32) for k in range(2)]

        for k in range(2):
            at = slice(k * half, (k + 1) * half)
            pair_mix[k].wait()
            aps[at] = (mixed[k].reshape(half, own_rows, -1) + apr[at].astype(F32)).astype(BF16)
            if k == 0:
                ring(0, 0).start()
                ring(0, 1).start()

    @pl.when(z < nz // 2)
    def _():
        project_heads()

    r, q = iota((slots, slots), 0), iota((slots, slots), 1)
    source = lax.rem(r, n_ep) * 16 + lax.rem(lax.div(r, n_ep), 2) * 8 + lax.div(r, rows)
    turn = jnp.where(q == source, 1.0, 0.0).astype(BF16)
    drain(darr.at[c, 0 : (n_ep - 1) * 16], drecv)
    pair_rows = remote(darr.at[c], darr.at[c], pair_s.at[4], pair_r.at[4], {"tp": other})
    pair_rows.start()
    pair_rows.wait()

    turned = nn(turn, jnp.concatenate([darr[0], darr[1]], axis=1)).astype(BF16)
    rows_in = jnp.concatenate(
        [
            turned[j * rows : (j + 1) * rows, h * width : (h + 1) * width]
            for h in range(2)
            for j in range(GROUPS)
        ],
        axis=1,
    )
    ready(16, 18)
    g, u = nn(rows_in, rg[...]), nn(rows_in, ru[...])
    hidden = (g * sigmoid(g) * u).astype(BF16)
    ready(18, 19)
    routed = nn(hidden, rd[...]).astype(BF16)
    for k in range(2 * GROUPS):
        ep[k % 2, k // 2] = routed[:, k * cols : (k + 1) * cols]
    pair_routed = remote(ep.at[1 - c], epr, pair_s.at[1], pair_r.at[1], {"tp": other})
    pair_routed.start()

    pair_routed.wait()
    es[...] = (ep[c].astype(F32) + epr[...].astype(F32)).astype(BF16)
    rb[y] = es[y]
    for k, d in enumerate(FAR_FIRST):
        to = lax.rem(y + d, GROUPS)
        y_sends.append(
            remote(es.at[to], rb.at[y], ysend.at[1, k], yrecv.at[1, k], {"tp": 2 * to + c})
        )
        y_sends[-1].start()

    @pl.when(z >= nz // 2)
    def _():
        project_heads()

    @pl.when(z < nz // 2)
    def _():
        ring_on(1)

    for copy in y_sends[GROUPS - 1 :]:
        copy.wait()
    every = jnp.concatenate([rb[k] for k in range(GROUPS)], axis=0)
    rout[...] = nn(back, every).astype(BF16)
    rarr[own, :] = rout[own, :]

    to_all(rout, rarr.at[own], rsend, rrecv, (*far_z, 0))

    @pl.when(z >= nz // 2)
    def _():
        ring_on(1)

    ring_on(2)
    ring_on(3)

    ready(20, 21)
    ring(2, 0).wait_recv()
    ring(3, 1).wait_recv()
    mix = aps[GROUPS - 1].astype(F32) + ring_in[2].astype(F32) + ring_in[6].astype(F32)
    scale = lax.rsqrt(jnp.mean(mix * mix, axis=1, keepdims=True) + NORM_EPSILON)
    out_a[...] = (mix * scale * png[...]).astype(BF16)

    for copy in y_sends[: GROUPS - 1]:
        copy.wait()
    drain(rarr.at[0 : (n_ep - 1) * 16], rrecv)
    answer = mm(weight, rarr[...])
    for k in range(GROUPS):
        answer = answer + sb[k].astype(F32)
    out_b[...] = answer.astype(BF16)


    for d in range(1, nz):
        @pl.when(z + d < nz)
        def _():
            drain(zs, zsend.at[d - 1])
    for way in range(2):
        for step in range(3 + way):
            ring(step, way).wait_send()
    drain(dout.at[0 : (n_ep - 1) * 16], dsend)
    drain(rout.at[0 : (n_ep - 1) * 16], rsend)


def solution(mesh):
    n_ep = mesh.shape["ep"]
    nx = 4 if n_ep % 4 == 0 else n_ep
    nz = n_ep // nx

    def body(rec, key, val, dec, lrn, gat, dco, spk, hng, how, png, exr, eng, idx, wts,
             rg, ru, rd, cg, cu, cd):
        ta, d = rec.shape[0], how.shape[1]
        tb = exr.shape[0]
        own, cols = ta // (2 * GROUPS), d // (2 * GROUPS)
        rows = n_ep * CAP
        width = d // (2 * GROUPS)
        line = lambda a: a.reshape(1, -1)
        given = [
            exr, line(eng), idx.T, cg.T, cu.T, cd, rec.T, key.T, val.T, dec.T, lrn.T, spk.T,
            line(dco), gat.T, line(hng), wts.T, rg[0], ru[0], rd[0], how, line(png),
        ]
        held = [pltpu.VMEM(a.shape, a.dtype) for a in given]
        held[3:5] = [pltpu.VMEM((2 * HC, d), BF16)]
        hbm = pl.BlockSpec(memory_space=pltpu.HBM)
        vmem = pl.BlockSpec(memory_space=pltpu.VMEM)
        given = [pltpu.with_memory_space_constraint(a, pltpu.HBM) for a in given]
        dma = pltpu.SemaphoreType.DMA
        return pl.pallas_call(
            functools.partial(kernel, nx, nz),
            out_shape=(
                jax.ShapeDtypeStruct((own, d), BF16),
                jax.ShapeDtypeStruct((tb, cols), BF16),
            ),
            in_specs=[hbm] * len(given),
            out_specs=(vmem, vmem),
            scratch_shapes=[
                *held,
                pltpu.VMEM((tb, d), BF16),
                pltpu.VMEM((n_ep * 16, width), BF16),
                pltpu.VMEM((2, n_ep * 16, width), BF16),
                pltpu.VMEM((2, GROUPS, rows, cols), BF16),
                pltpu.VMEM((GROUPS, rows, cols), BF16),
                pltpu.VMEM((GROUPS, rows, cols), BF16),
                pltpu.VMEM((GROUPS, rows, cols), BF16),
                pltpu.VMEM((n_ep * 16, cols), BF16),
                pltpu.VMEM((n_ep * 16, cols), BF16),
                pltpu.VMEM((2, GROUPS, tb, cols), BF16),
                pltpu.VMEM((GROUPS, tb, cols), BF16),
                pltpu.VMEM((GROUPS, tb, cols), BF16),
                pltpu.VMEM((GROUPS, tb, cols), BF16),
                pltpu.VMEM((GROUPS, 2, own, HC), BF16),
                pltpu.VMEM((GROUPS, own, d), BF16),
                pltpu.VMEM((GROUPS, own, d), BF16),
                pltpu.VMEM((GROUPS, own, d), BF16),
                pltpu.VMEM((GROUPS - 1, own, d), BF16),
                pltpu.VMEM((nx, HC, 2 * HC), BF16),
                pltpu.VMEM((HC, 2 * HC), BF16),
                pltpu.VMEM((nz, HC, 2 * HC), BF16),
                dma((len(given),)),
                dma((5,)),
                dma((5,)),
                dma,
                dma,
                dma((2, GROUPS - 1)),
                dma((2, GROUPS - 1)),
                dma((7,)),
                dma((7,)),
                dma,
                dma,
                dma((max(nx - 1, 1),)),
                dma((max(nx - 1, 1),)),
                dma((max(nz - 1, 1),)),
                dma((max(nz, 1),)),
                pltpu.VMEM((2 * HC, ta), F32),
            ],
            compiler_params=pltpu.CompilerParams(
                collective_id=0, has_side_effects=True, vmem_limit_bytes=48 * 1024 * 1024
            ),
        )(*given)

    placed = (
        P("ep", "tp"), P("ep", "tp"), P("ep", "tp"), P("ep", "tp"), P("ep", "tp"), P("ep", "tp"),
        P("tp"), P("ep", "tp"), P("tp"), P("tp", None), P(), P("ep", None), P(), P("ep", None),
        P("ep", None), P(("ep", "tp"), None, None), P(("ep", "tp"), None, None),
        P(("ep", "tp"), None, None), P(None, "tp"), P(None, "tp"), P("tp", None),
    )
    return jax.shard_map(
        body,
        mesh=mesh,
        in_specs=placed,
        out_specs=(P(("ep", "tp"), None), P("ep", "tp")),
        check_vma=False,
    )
```

```python
import functools
import math

import jax
import jax.numpy as jnp
from jax import lax
from jax.experimental import pallas as pl
from jax.experimental.pallas import tpu as pltpu
from jax.sharding import PartitionSpec as P

HC = 64
L = 128
GROUPS = 8
CAP = 2
FAR_FIRST = (4, 3, 5, 2, 6, 1, 7)
NORM_EPSILON = 1e-06
GROUP_EPSILON = 0.00064
F32 = jnp.float32
BF16 = jnp.bfloat16
MESH = pl.DeviceIdType.MESH


def nn(a, b):
    return jnp.dot(a, b, preferred_element_type=F32)


def nt(a, b):
    return lax.dot_general(a, b, (((1,), (1,)), ((), ())), preferred_element_type=F32)


def parts(a, count):
    out = []
    for k in range(count):
        piece = a.astype(BF16)
        out.append(piece)
        if k < count - 1:
            a = a - piece.astype(F32)
    return out


def mm(a, b, product=nn, na=2, nb=2):
    pa = [a] if a.dtype == BF16 else parts(a, na)
    pb = [b] if b.dtype == BF16 else parts(b, nb)
    total = None
    for i, x in enumerate(pa):
        for j, y in enumerate(pb):
            if i + j < max(len(pa), len(pb)):
                term = product(x, y)
                total = term if total is None else total + term
    return total


def square(a, b):
    (ah, al), (bh, bl) = parts(a, 2), parts(b, 2)
    both = nn(
        jnp.concatenate([ah, al], axis=1),
        jnp.concatenate(
            [
                jnp.concatenate([bh, bl], axis=1),
                jnp.concatenate([bh, jnp.zeros_like(bl)], axis=1),
            ],
            axis=0,
        ),
    )
    return both[:, :L] + both[:, L:]


def iota(shape, dim):
    return lax.broadcasted_iota(jnp.int32, shape, dim)


def sigmoid(v):
    return 1.0 / (1.0 + jnp.exp(-v))


def column(row):
    n = row.shape[1]
    return jnp.sum(
        jnp.where(iota((n, n), 0) == iota((n, n), 1), row, 0.0), axis=1, keepdims=True
    )


def beside_identity(f):
    top = jnp.where(iota((HC, 2 * HC), 0) == iota((HC, 2 * HC), 1), 1.0, 0.0)
    return jnp.concatenate([top.astype(f.dtype), f], axis=0)


def joined(late, early):
    return mm(late, beside_identity(early))


def solved(right, n):
    r, c = iota((L, L), 0), iota((L, L), 1)
    eye = jnp.where(r == c, 1.0, 0.0)
    same8 = r // 8 == c // 8
    same32 = r // 32 == c // 32
    small = jnp.where(same8, n, 0.0)
    middle = jnp.where(same32 & (r // 8 != c // 8), n, 0.0)
    large = jnp.where(same32, 0.0, n)
    two = square(small, small)
    four = square(two, two)
    first = eye + small + two + square(small, two)
    x = first + square(first, four)
    step = square(middle, x)
    x = x + square(x, step)
    x = x + square(x, square(step, step))
    step = square(large, x)
    y = square(right, x)
    y = y + square(y, step)
    return y + square(y, square(step, step))


def local_block(rec, key, val, removal, lr, ld):
    s, t = iota((L, L), 0), iota((L, L), 1)
    upto = jnp.where(s <= t, 1.0, 0.0).astype(BF16)
    cum = sum(nn(p, upto) for p in parts(ld, 3))
    ref, end = cum[:, L // 2 - 1 : L // 2], cum[:, L - 1 : L]
    eq = jnp.exp(cum - ref)
    eb = jnp.exp(cum - ld - ref)
    ek = jnp.exp(ref - cum)
    eref, eend = jnp.exp(ref), jnp.exp(end - ref)
    qn, qr = -removal * eb, rec * eq
    kb, kk = removal * lr * ek, key * lr * ek
    keys = jnp.concatenate([kb.T, kk.T], axis=0)
    both = mm(keys, jnp.concatenate([qn, qr], axis=1))
    lb = jnp.where(s < t, both[:L, :L], 0.0)
    ob = jnp.where(s <= t, both[:L, L:], 0.0)
    lk = jnp.where(s < t, both[L:, :L], 0.0)
    ok = jnp.where(s <= t, both[L:, L:], 0.0)
    return lb, ob, lk, ok, kb, kk, qn, qr, eref, eend, jnp.exp(end), val


def local_result(lb, ob, lk, ok, kb, kk, qn, qr, eref, eend, whole, val):
    valued = mm(val, jnp.concatenate([lk, ok], axis=1))
    right = jnp.concatenate([valued[:, :L], qn * eref], axis=0)
    corr = solved(right, lb)
    z = square(corr, ob) + jnp.concatenate([valued[:, L:], qr * eref], axis=0)
    aug = jnp.concatenate([val, jnp.zeros_like(val)], axis=0)
    f = mm(
        jnp.concatenate([kb * eend, kk * eend], axis=1),
        jnp.concatenate([corr, aug.astype(F32)], axis=1),
        nt,
    )
    f = f + jnp.where(
        iota((HC, 2 * HC), 0) + HC == iota((HC, 2 * HC), 1), whole, 0.0
    )
    return f, z


def kernel(nx, nz, *refs):
    from_hbm = refs[:21]
    out_a, out_b = refs[21:23]
    (exr, eng, idx, cgu, cd, rec, key, val, dec, lrn, spk, dco, gat, hng, wts, rg, ru, rd, how, png, nb, dout, darr, ep, epr, es, rarr,
     sp, spr, ss, sb, ho, ap, apr, aps, ring_in, xarr, zs, zarr, load, pair_s, pair_r, dsend, drecv,
     seen, ysend, yrecv, rsum_s, rsum_r, rsend, rrecv, xsend, xrecv, zsend, zrecv, zsc) = refs[23:]
    n_ep = nx * nz
    tb = exr.shape[0]
    rows = n_ep * CAP
    slots = rows * GROUPS
    me, t = lax.axis_index("ep"), lax.axis_index("tp")
    y, c = lax.div(t, 2), lax.rem(t, 2)
    z, x = lax.div(me, nx), lax.rem(me, nx)
    other = t + 1 - 2 * c

    def remote(src, dst, send, recv, where):
        return pltpu.make_async_remote_copy(
            src_ref=src, dst_ref=dst, send_sem=send, recv_sem=recv,
            device_id=where, device_id_type=MESH,
        )

    def drain(ref, sem):
        pltpu.make_async_copy(ref, ref, sem).wait()

    def ready(start, stop):
        for copy in loads[start:stop]:
            copy.wait()

    targets = (
        exr, eng, idx, cgu.at[0:HC], cgu.at[HC : 2 * HC], cd, rec, key, val, dec, lrn, spk, dco,
        gat, hng, wts, rg, ru, rd, how, png,
    )
    loads = [
        pltpu.make_async_copy(a, b, load.at[k])
        for k, (a, b) in enumerate(zip(from_hbm, targets, strict=True))
    ]
    for copy in loads[:3]:
        copy.start()

    unit = jnp.where(iota((HC, 2 * HC), 0) + HC == iota((HC, 2 * HC), 1), 1.0, 0.0)
    for k in range(nz):
        zarr[k] = unit.astype(BF16)

    barrier = pltpu.get_barrier_semaphore()

    def greet(semaphore, where):
        pl.semaphore_signal(semaphore, inc=1, device_id=where, device_id_type=MESH)

    def greet_ep(d, carry):
        greet(barrier, {"ep": lax.rem(me + d, n_ep)})
        return carry

    lax.fori_loop(n_ep // 2, n_ep, greet_ep, 0)
    lax.fori_loop(1, n_ep // 2, greet_ep, 0)
    for d in FAR_FIRST:
        greet(barrier, {"tp": 2 * lax.rem(y + d, GROUPS) + c})
    greet(barrier, {"tp": other})

    for k in (*range(6, 13), *range(3, 6), *range(16, 20), *range(13, 16), 20):
        loads[k].start()
    ready(2, 3)
    first, second = idx[0:1, :], idx[1:2, :]
    i = iota((rows, tb), 0)
    expert = lax.div(i, CAP) * GROUPS + y
    hits = jnp.where((first == expert) | (second == expert), 1.0, 0.0)
    earlier = jnp.where(iota((tb, tb), 0) < iota((tb, tb), 1), 1.0, 0.0).astype(BF16)
    rank = nn(hits.astype(BF16), earlier)
    picks = jnp.where(rank == lax.rem(i, CAP).astype(F32), hits, 0.0).astype(BF16)

    ready(0, 2)
    wide = exr[...].astype(F32)
    scale = lax.rsqrt(jnp.mean(wide * wide, axis=1, keepdims=True) + NORM_EPSILON)
    nb[...] = (wide * scale * eng[...]).astype(BF16)

    width = dout.shape[2]
    mine = nb[:, pl.ds(pl.multiple_of(c * width, width), width)]
    dout[...] = nn(picks, mine).reshape(n_ep, CAP, width).astype(BF16)
    darr[c, me] = dout[me]

    def offsets():
        return [(zo, xo) for zo in (*far_z, 0) for xo in far_x]

    far_z = sorted(range(1, nz), key=lambda v: -min(v, nz - v))
    far_x = sorted(range(nx), key=lambda v: -min(v, nx - v))

    pair_shared = remote(sp.at[1 - c], spr, pair_s.at[0], pair_r.at[0], {"tp": other})

    def meet():
        pl.semaphore_wait(barrier, GROUPS + n_ep - 1)
        for d in FAR_FIRST:
            greet(seen, {"tp": 2 * lax.rem(y + d, GROUPS) + c})
        for zo, xo in offsets():
            if zo or xo:
                to = lax.rem(z + zo, nz) * nx + lax.rem(x + xo, nx)
                remote(dout.at[to], darr.at[c, me], dsend, drecv, {"ep": to}).start()

    @pl.when(z >= nz // 2)
    def _():
        meet()

    ready(6, 13)
    k_in = key[...].astype(F32)
    pre = column(dco[...]) + jnp.tanh(dec[...].astype(F32))
    ld = spk[...] - sigmoid(pre) * math.exp(-0.5)
    lr = sigmoid(lrn[...].astype(F32))
    removal = k_in * lax.rsqrt(jnp.sum(k_in * k_in, axis=0, keepdims=True) + NORM_EPSILON)
    r_in = rec[...].astype(F32)
    prepared = []
    for b in range(key.shape[1] // L):
        at = slice(b * L, (b + 1) * L)
        prepared.append(
            local_block(r_in[:, at], k_in[:, at], val[:, at], removal[:, at], lr[:, at], ld[:, at])
        )

    ready(3, 6)
    gate_up = nt(cgu[...], nb[...])
    g, u = gate_up[:HC], gate_up[HC:]
    hidden = (g * sigmoid(g) * u).T.astype(BF16)
    shared = nn(hidden, cd[...]).astype(BF16)
    cols = shared.shape[1] // (2 * GROUPS)
    for k in range(2 * GROUPS):
        sp[k % 2, k // 2] = shared[:, k * cols : (k + 1) * cols]

    @pl.when(z >= nz // 2)
    def _():
        pair_shared.start()

    blocks = [local_result(*values) for values in prepared]
    f, z_out = blocks[0]
    z_all = [z_out]
    for later_f, later_z in blocks[1:]:
        z_all.append(mm(beside_identity(f).T, later_z))
        f = joined(later_f, f)
    z_all = jnp.concatenate(z_all, axis=1)
    xarr[x] = f.astype(BF16)

    @pl.when(z < nz // 2)
    def _():
        meet()
        pair_shared.start()

    x_sends = [
        remote(
            xarr.at[x], xarr.at[x], xsend.at[d - 1], xrecv.at[d - 1],
            {"ep": z * nx + lax.rem(x + d, nx)},
        )
        for d in range(1, nx)
    ]
    for copy in x_sends:
        copy.start()

    ready(13, 16)
    lines = jnp.concatenate(
        [first.astype(F32), second.astype(F32), wts[...], jnp.zeros((4, tb), F32)], axis=0
    ).T
    q = iota((tb, slots), 1)
    expert = (lax.div(q, 16) * GROUPS + lax.div(lax.rem(q, 16), 2)).astype(F32)
    hit_a = jnp.where(lines[:, 0:1] == expert, 1.0, 0.0)
    hit_b = jnp.where(lines[:, 1:2] == expert, 1.0, 0.0)
    earlier = jnp.where(iota((tb, tb), 0) > iota((tb, tb), 1), 1.0, 0.0).astype(BF16)
    rank = nn(earlier, (hit_a + hit_b).astype(BF16))
    weight = jnp.where(
        rank == lax.rem(q, 2).astype(F32), hit_a * lines[:, 2:3] + hit_b * lines[:, 3:4], 0.0
    )

    pair_shared.wait()
    ss[...] = (sp[c].astype(F32) + spr[...].astype(F32)).astype(BF16)
    sb[y] = ss[y]
    y_sends = []
    for k, d in enumerate(FAR_FIRST):
        to = lax.rem(y + d, GROUPS)
        y_sends.append(
            remote(ss.at[to], sb.at[y], ysend.at[k], yrecv.at[k], {"tp": 2 * to + c})
        )
        y_sends[-1].start()

    for copy in x_sends:
        copy.wait()
    stretch = [xarr[k] for k in range(nx)]
    before = unit
    total = stretch[0]
    for k in range(1, nx):
        before = jnp.where(x == k, total.astype(F32), before)
        total = joined(stretch[k], total)
    zs[...] = total.astype(BF16)
    for d in range(1, nz):
        @pl.when(z + d < nz)
        def _():
            remote(
                zs, zarr.at[z], zsend.at[d - 1], zrecv.at[z], {"ep": (z + d) * nx + x}
            ).start()

    zsc[...] = mm(beside_identity(before).T, z_all)

    order = FAR_FIRST + (0,)

    def ring(step, way):
        k = 3 * way + step
        to = lax.rem(y + (GROUPS - 1 if way else 1), GROUPS)
        slot = order.index(4 + step if way else 3 - step)
        return remote(aps.at[slot], ring_in.at[k], rsum_s.at[k], rsum_r.at[k], {"tp": 2 * to + c})

    def ring_on(step):
        for way in range(2):
            if step < 3 + way:
                ring(step - 1, way).wait_recv()
                slot = order.index(4 + step if way else 3 - step)
                arrived = ring_in[3 * way + step - 1].astype(F32)
                aps[slot] = (aps[slot].astype(F32) + arrived).astype(BF16)
                ring(step, way).start()

    def project_heads():
        for k in range(nz - 1):
            @pl.when(k < z)
            def _():
                drain(zarr.at[k], zrecv.at[k])

        level = [zarr[k] for k in range(nz - 1)] if nz > 1 else [unit.astype(BF16)]
        while len(level) > 1:
            nxt = [joined(level[k + 1], level[k]) for k in range(0, len(level) - 1, 2)]
            if len(level) % 2:
                nxt.append(level[-1].astype(F32))
            level = nxt

        carried = level[0].astype(F32)
        head = mm(beside_identity(carried).T[:HC], zsc[...])
        centred = head - jnp.mean(head, axis=0, keepdims=True)
        normed = centred * lax.rsqrt(jnp.mean(centred * centred, axis=0, keepdims=True) + GROUP_EPSILON)
        heads_out = normed * column(hng[...]) * sigmoid(gat[...].astype(F32))
        heads_out = heads_out.T.astype(BF16)
        own_rows = out_a.shape[0]
        ho[...] = heads_out.reshape(GROUPS, 2, own_rows, HC)
        ready(19, 20)

        half = GROUPS // 2

        def product(first, core):
            lines = [ho[lax.rem(y + d, GROUPS), core] for d in order[first : first + half]]
            return nn(jnp.concatenate(lines, axis=0), how[...])

        pair_mix = []
        for k in range(2):
            at = slice(k * half, (k + 1) * half)
            ap[at] = product(k * half, 1 - c).astype(BF16).reshape(half, own_rows, -1)
            pair_mix.append(
                remote(ap.at[at], apr.at[at], pair_s.at[2 + k], pair_r.at[2 + k], {"tp": other})
            )
            pair_mix[-1].start()
        mixed = [product(k * half, c).astype(BF16).astype(F32) for k in range(2)]

        for k in range(2):
            at = slice(k * half, (k + 1) * half)
            pair_mix[k].wait()
            aps[at] = (mixed[k].reshape(half, own_rows, -1) + apr[at].astype(F32)).astype(BF16)
            if k == 0:
                ring(0, 0).start()
                ring(0, 1).start()

    @pl.when(z < nz // 2)
    def _():
        project_heads()

    drain(darr.at[c, 0 : n_ep - 1], drecv)
    pair_rows = remote(darr.at[c], darr.at[c], pair_s.at[4], pair_r.at[4], {"tp": other})
    pair_rows.start()
    pair_rows.wait()

    rows_in = jnp.concatenate([darr[h].reshape(rows, width) for h in range(2)], axis=1)
    ready(16, 18)
    g, u = nn(rows_in, rg[...]), nn(rows_in, ru[...])
    hidden = (g * sigmoid(g) * u).astype(BF16)
    ready(18, 19)
    routed = nn(hidden, rd[...]).astype(BF16)
    for k in range(2 * GROUPS):
        ep[k % 2, k // 2] = routed[:, k * cols : (k + 1) * cols]
    pair_routed = remote(ep.at[1 - c], epr, pair_s.at[1], pair_r.at[1], {"tp": other})
    pair_routed.start()

    pair_routed.wait()
    both = ep[c].astype(F32) + epr[...].astype(F32)
    es[...] = both.reshape(GROUPS * n_ep, CAP, cols).astype(BF16)
    place = me * GROUPS + y
    rarr[place] = es[y * n_ep + me]
    pl.semaphore_wait(seen, GROUPS - 1)

    def send_back(k, carry):
        yo = lax.rem(y + GROUPS // 2 + k, GROUPS)
        for zo, xo in offsets():
            to = lax.rem(z + zo, nz) * nx + lax.rem(x + xo, nx)
            copy = remote(
                es.at[yo * n_ep + to], rarr.at[place], rsend, rrecv, {"ep": to, "tp": 2 * yo + c}
            )
            if zo or xo:
                copy.start()
            else:
                pl.when(yo != y)(copy.start)
        return carry

    lax.fori_loop(0, GROUPS, send_back, 0)

    @pl.when(z >= nz // 2)
    def _():
        project_heads()

    ring_on(1)
    ring_on(2)
    ring_on(3)

    ready(20, 21)
    ring(2, 0).wait_recv()
    ring(3, 1).wait_recv()
    mix = aps[GROUPS - 1].astype(F32) + ring_in[2].astype(F32) + ring_in[6].astype(F32)
    scale = lax.rsqrt(jnp.mean(mix * mix, axis=1, keepdims=True) + NORM_EPSILON)
    out_a[...] = (mix * scale * png[...]).astype(BF16)

    for copy in y_sends:
        copy.wait()
    drain(rarr.at[0 : n_ep * GROUPS - 1], rrecv)
    answer = mm(weight, rarr[...].reshape(slots, cols))
    for k in range(GROUPS):
        answer = answer + sb[k].astype(F32)
    out_b[...] = answer.astype(BF16)


    for d in range(1, nz):
        @pl.when(z + d < nz)
        def _():
            drain(zs, zsend.at[d - 1])
    for way in range(2):
        for step in range(3 + way):
            ring(step, way).wait_send()
    drain(dout.at[0 : n_ep - 1], dsend)
    drain(es.at[0 : n_ep * GROUPS - 1], rsend)


def solution(mesh):
    n_ep = mesh.shape["ep"]
    nx = 4 if n_ep % 4 == 0 else n_ep
    nz = n_ep // nx

    def body(rec, key, val, dec, lrn, gat, dco, spk, hng, how, png, exr, eng, idx, wts,
             rg, ru, rd, cg, cu, cd):
        ta, d = rec.shape[0], how.shape[1]
        tb = exr.shape[0]
        own, cols = ta // (2 * GROUPS), d // (2 * GROUPS)
        rows = n_ep * CAP
        line = lambda a: a.reshape(1, -1)
        given = [
            exr, line(eng), idx.T, cg.T, cu.T, cd, rec.T, key.T, val.T, dec.T, lrn.T, spk.T,
            line(dco), gat.T, line(hng), wts.T, rg[0], ru[0], rd[0], how, line(png),
        ]
        held = [pltpu.VMEM(a.shape, a.dtype) for a in given]
        held[3:5] = [pltpu.VMEM((2 * HC, d), BF16)]
        hbm = pl.BlockSpec(memory_space=pltpu.HBM)
        vmem = pl.BlockSpec(memory_space=pltpu.VMEM)
        given = [pltpu.with_memory_space_constraint(a, pltpu.HBM) for a in given]
        dma = pltpu.SemaphoreType.DMA
        return pl.pallas_call(
            functools.partial(kernel, nx, nz),
            out_shape=(
                jax.ShapeDtypeStruct((own, d), BF16),
                jax.ShapeDtypeStruct((tb, cols), BF16),
            ),
            in_specs=[hbm] * len(given),
            out_specs=(vmem, vmem),
            scratch_shapes=[
                *held,
                pltpu.VMEM((tb, d), BF16),
                pltpu.VMEM((n_ep, CAP, d // 2), BF16),
                pltpu.VMEM((2, n_ep, CAP, d // 2), BF16),
                pltpu.VMEM((2, GROUPS, rows, cols), BF16),
                pltpu.VMEM((GROUPS, rows, cols), BF16),
                pltpu.VMEM((GROUPS * n_ep, CAP, cols), BF16),
                pltpu.VMEM((GROUPS * n_ep, CAP, cols), BF16),
                pltpu.VMEM((2, GROUPS, tb, cols), BF16),
                pltpu.VMEM((GROUPS, tb, cols), BF16),
                pltpu.VMEM((GROUPS, tb, cols), BF16),
                pltpu.VMEM((GROUPS, tb, cols), BF16),
                pltpu.VMEM((GROUPS, 2, own, HC), BF16),
                pltpu.VMEM((GROUPS, own, d), BF16),
                pltpu.VMEM((GROUPS, own, d), BF16),
                pltpu.VMEM((GROUPS, own, d), BF16),
                pltpu.VMEM((GROUPS - 1, own, d), BF16),
                pltpu.VMEM((nx, HC, 2 * HC), BF16),
                pltpu.VMEM((HC, 2 * HC), BF16),
                pltpu.VMEM((nz, HC, 2 * HC), BF16),
                dma((len(given),)),
                dma((5,)),
                dma((5,)),
                dma,
                dma,
                pltpu.SemaphoreType.REGULAR,
                dma((GROUPS - 1,)),
                dma((GROUPS - 1,)),
                dma((7,)),
                dma((7,)),
                dma,
                dma,
                dma((max(nx - 1, 1),)),
                dma((max(nx - 1, 1),)),
                dma((max(nz - 1, 1),)),
                dma((max(nz, 1),)),
                pltpu.VMEM((2 * HC, ta), F32),
            ],
            compiler_params=pltpu.CompilerParams(
                collective_id=0, has_side_effects=True, vmem_limit_bytes=48 * 1024 * 1024
            ),
        )(*given)

    placed = (
        P("ep", "tp"), P("ep", "tp"), P("ep", "tp"), P("ep", "tp"), P("ep", "tp"), P("ep", "tp"),
        P("tp"), P("ep", "tp"), P("tp"), P("tp", None), P(), P("ep", None), P(), P("ep", None),
        P("ep", None), P(("ep", "tp"), None, None), P(("ep", "tp"), None, None),
        P(("ep", "tp"), None, None), P(None, "tp"), P(None, "tp"), P("tp", None),
    )
    return jax.shard_map(
        body,
        mesh=mesh,
        in_specs=placed,
        out_specs=(P(("ep", "tp"), None), P("ep", "tp")),
        check_vma=False,
    )
```

```python
import functools
import math

import jax
import jax.numpy as jnp
from jax import lax
from jax.experimental import pallas as pl
from jax.experimental.pallas import tpu as pltpu
from jax.sharding import PartitionSpec as P

HC = 64
L = 128
GROUPS = 8
CAP = 2
FAR_FIRST = (4, 3, 5, 2, 6, 1, 7)
NORM_EPSILON = 1e-06
GROUP_EPSILON = 0.00064
F32 = jnp.float32
BF16 = jnp.bfloat16
MESH = pl.DeviceIdType.MESH


def nn(a, b):
    return jnp.dot(a, b, preferred_element_type=F32)


def nt(a, b):
    return lax.dot_general(a, b, (((1,), (1,)), ((), ())), preferred_element_type=F32)


def parts(a, count):
    out = []
    for k in range(count):
        piece = a.astype(BF16)
        out.append(piece)
        if k < count - 1:
            a = a - piece.astype(F32)
    return out


def mm(a, b, product=nn, na=2, nb=2):
    pa = [a] if a.dtype == BF16 else parts(a, na)
    pb = [b] if b.dtype == BF16 else parts(b, nb)
    total = None
    for i, x in enumerate(pa):
        for j, y in enumerate(pb):
            if i + j < max(len(pa), len(pb)):
                term = product(x, y)
                total = term if total is None else total + term
    return total


def square(a, b):
    (ah, al), (bh, bl) = parts(a, 2), parts(b, 2)
    both = nn(
        jnp.concatenate([ah, al], axis=1),
        jnp.concatenate(
            [
                jnp.concatenate([bh, bl], axis=1),
                jnp.concatenate([bh, jnp.zeros_like(bl)], axis=1),
            ],
            axis=0,
        ),
    )
    return both[:, :L] + both[:, L:]


def iota(shape, dim):
    return lax.broadcasted_iota(jnp.int32, shape, dim)


def sigmoid(v):
    return 1.0 / (1.0 + jnp.exp(-v))


def column(row):
    n = row.shape[1]
    return jnp.sum(
        jnp.where(iota((n, n), 0) == iota((n, n), 1), row, 0.0), axis=1, keepdims=True
    )


def beside_identity(f):
    top = jnp.where(iota((HC, 2 * HC), 0) == iota((HC, 2 * HC), 1), 1.0, 0.0)
    return jnp.concatenate([top.astype(f.dtype), f], axis=0)


def joined(late, early):
    return mm(late, beside_identity(early))


def solved(right, n):
    r, c = iota((L, L), 0), iota((L, L), 1)
    eye = jnp.where(r == c, 1.0, 0.0)
    same8 = r // 8 == c // 8
    same32 = r // 32 == c // 32
    small = jnp.where(same8, n, 0.0)
    middle = jnp.where(same32 & (r // 8 != c // 8), n, 0.0)
    large = jnp.where(same32, 0.0, n)
    two = square(small, small)
    four = square(two, two)
    first = eye + small + two + square(small, two)
    x = first + square(first, four)
    step = square(middle, x)
    x = x + square(x, step)
    x = x + square(x, square(step, step))
    step = square(large, x)
    y = square(right, x)
    y = y + square(y, step)
    return y + square(y, square(step, step))


def local_block(rec, key, val, removal, lr, ld):
    s, t = iota((L, L), 0), iota((L, L), 1)
    upto = jnp.where(s <= t, 1.0, 0.0).astype(BF16)
    cum = sum(nn(p, upto) for p in parts(ld, 3))
    ref, end = cum[:, L // 2 - 1 : L // 2], cum[:, L - 1 : L]
    eq = jnp.exp(cum - ref)
    eb = jnp.exp(cum - ld - ref)
    ek = jnp.exp(ref - cum)
    eref, eend = jnp.exp(ref), jnp.exp(end - ref)
    qn, qr = -removal * eb, rec * eq
    kb, kk = removal * lr * ek, key * lr * ek
    keys = jnp.concatenate([kb.T, kk.T], axis=0)
    both = mm(keys, jnp.concatenate([qn, qr], axis=1))
    lb = jnp.where(s < t, both[:L, :L], 0.0)
    ob = jnp.where(s <= t, both[:L, L:], 0.0)
    lk = jnp.where(s < t, both[L:, :L], 0.0)
    ok = jnp.where(s <= t, both[L:, L:], 0.0)
    return lb, ob, lk, ok, kb, kk, qn, qr, eref, eend, jnp.exp(end), val


def local_result(lb, ob, lk, ok, kb, kk, qn, qr, eref, eend, whole, val):
    valued = mm(val, jnp.concatenate([lk, ok], axis=1))
    right = jnp.concatenate([valued[:, :L], qn * eref], axis=0)
    corr = solved(right, lb)
    z = square(corr, ob) + jnp.concatenate([valued[:, L:], qr * eref], axis=0)
    aug = jnp.concatenate([val, jnp.zeros_like(val)], axis=0)
    f = mm(
        jnp.concatenate([kb * eend, kk * eend], axis=1),
        jnp.concatenate([corr, aug.astype(F32)], axis=1),
        nt,
    )
    f = f + jnp.where(
        iota((HC, 2 * HC), 0) + HC == iota((HC, 2 * HC), 1), whole, 0.0
    )
    return f, z


def kernel(nx, nz, *refs):
    from_hbm = refs[:21]
    out_a, out_b = refs[21:23]
    (exr, eng, idx, cgu, cd, rec, key, val, dec, lrn, spk, dco, gat, hng, wts, rg, ru, rd, how, png, nb, dout, darr, ep, epr, es, rarr,
     sp, spr, ss, sb, ho, ap, apr, aps, ring_in, xarr, zs, zarr, load, pair_s, pair_r, dsend, drecv,
     seen, ysend, yrecv, rsum_s, rsum_r, rsend, rrecv, xsend, xrecv, zsend, zrecv, zsc) = refs[23:]
    n_ep = nx * nz
    tb = exr.shape[0]
    rows = n_ep * CAP
    slots = rows * GROUPS
    me, t = lax.axis_index("ep"), lax.axis_index("tp")
    y, c = lax.div(t, 2), lax.rem(t, 2)
    z, x = lax.div(me, nx), lax.rem(me, nx)
    other = t + 1 - 2 * c

    def remote(src, dst, send, recv, where):
        return pltpu.make_async_remote_copy(
            src_ref=src, dst_ref=dst, send_sem=send, recv_sem=recv,
            device_id=where, device_id_type=MESH,
        )

    def drain(ref, sem):
        pltpu.make_async_copy(ref, ref, sem).wait()

    def ready(start, stop):
        for copy in loads[start:stop]:
            copy.wait()

    targets = (
        exr, eng, idx, cgu.at[0:HC], cgu.at[HC : 2 * HC], cd, rec, key, val, dec, lrn, spk, dco,
        gat, hng, wts, rg, ru, rd, how, png,
    )
    loads = [
        pltpu.make_async_copy(a, b, load.at[k])
        for k, (a, b) in enumerate(zip(from_hbm, targets, strict=True))
    ]
    for copy in loads[:3]:
        copy.start()

    unit = jnp.where(iota((HC, 2 * HC), 0) + HC == iota((HC, 2 * HC), 1), 1.0, 0.0)
    for k in range(nz):
        zarr[k] = unit.astype(BF16)

    barrier = pltpu.get_barrier_semaphore()

    def greet(semaphore, where):
        pl.semaphore_signal(semaphore, inc=1, device_id=where, device_id_type=MESH)

    def greet_ep(d, carry):
        greet(barrier, {"ep": lax.rem(me + d, n_ep)})
        return carry

    lax.fori_loop(n_ep // 2, n_ep, greet_ep, 0)
    lax.fori_loop(1, n_ep // 2, greet_ep, 0)
    for d in FAR_FIRST:
        greet(barrier, {"tp": 2 * lax.rem(y + d, GROUPS) + c})
    greet(barrier, {"tp": other})

    for k in (*range(6, 13), *range(3, 6), *range(16, 20), *range(13, 16), 20):
        loads[k].start()
    ready(2, 3)
    choice_a, choice_b = idx[0:1, :], idx[1:2, :]
    i = iota((rows, tb), 0)
    expert = lax.div(i, CAP) * GROUPS + y
    hits = jnp.where((choice_a == expert) | (choice_b == expert), 1.0, 0.0)
    earlier = jnp.where(iota((tb, tb), 0) < iota((tb, tb), 1), 1.0, 0.0).astype(BF16)
    rank = nn(hits.astype(BF16), earlier)
    picks = jnp.where(rank == lax.rem(i, CAP).astype(F32), hits, 0.0).astype(BF16)

    ready(0, 2)
    wide = exr[...].astype(F32)
    scale = lax.rsqrt(jnp.mean(wide * wide, axis=1, keepdims=True) + NORM_EPSILON)
    nb[...] = (wide * scale * eng[...]).astype(BF16)

    width = dout.shape[2]
    mine = nb[:, pl.ds(pl.multiple_of(c * width, width), width)]
    dout[...] = nn(picks, mine).reshape(n_ep, CAP, width).astype(BF16)
    darr[c, me] = dout[me]

    def offsets():
        return [(zo, xo) for zo in (*far_z, 0) for xo in far_x]

    far_z = sorted(range(1, nz), key=lambda v: -min(v, nz - v))
    far_x = sorted(range(nx), key=lambda v: -min(v, nx - v))

    pair_shared = remote(sp.at[1 - c], spr, pair_s.at[0], pair_r.at[0], {"tp": other})

    def meet():
        pl.semaphore_wait(barrier, GROUPS + n_ep - 1)
        for d in FAR_FIRST:
            greet(seen, {"tp": 2 * lax.rem(y + d, GROUPS) + c})
        for zo, xo in offsets():
            if zo or xo:
                to = lax.rem(z + zo, nz) * nx + lax.rem(x + xo, nx)
                remote(dout.at[to], darr.at[c, me], dsend, drecv, {"ep": to}).start()

    last = (z >= nz // 2) & (y >= GROUPS // 2)
    first = (z < nz // 2) | (y == 0)

    @pl.when(last)
    def _():
        meet()

    ready(6, 13)
    k_in = key[...].astype(F32)
    pre = column(dco[...]) + jnp.tanh(dec[...].astype(F32))
    ld = spk[...] - sigmoid(pre) * math.exp(-0.5)
    lr = sigmoid(lrn[...].astype(F32))
    removal = k_in * lax.rsqrt(jnp.sum(k_in * k_in, axis=0, keepdims=True) + NORM_EPSILON)
    r_in = rec[...].astype(F32)
    prepared = []
    for b in range(key.shape[1] // L):
        at = slice(b * L, (b + 1) * L)
        prepared.append(
            local_block(r_in[:, at], k_in[:, at], val[:, at], removal[:, at], lr[:, at], ld[:, at])
        )

    ready(3, 6)
    gate_up = nt(cgu[...], nb[...])
    g, u = gate_up[:HC], gate_up[HC:]
    hidden = (g * sigmoid(g) * u).T.astype(BF16)
    shared = nn(hidden, cd[...]).astype(BF16)
    cols = shared.shape[1] // (2 * GROUPS)
    for k in range(2 * GROUPS):
        sp[k % 2, k // 2] = shared[:, k * cols : (k + 1) * cols]

    @pl.when(jnp.logical_not(last | first))
    def _():
        meet()

    @pl.when(jnp.logical_not(first))
    def _():
        pair_shared.start()

    blocks = [local_result(*values) for values in prepared]
    f, z_out = blocks[0]
    z_all = [z_out]
    for later_f, later_z in blocks[1:]:
        z_all.append(mm(beside_identity(f).T, later_z))
        f = joined(later_f, f)
    z_all = jnp.concatenate(z_all, axis=1)
    xarr[x] = f.astype(BF16)

    @pl.when(first)
    def _():
        meet()
        pair_shared.start()

    x_sends = [
        remote(
            xarr.at[x], xarr.at[x], xsend.at[d - 1], xrecv.at[d - 1],
            {"ep": z * nx + lax.rem(x + d, nx)},
        )
        for d in range(1, nx)
    ]
    for copy in x_sends:
        copy.start()

    ready(13, 16)
    lines = jnp.concatenate(
        [choice_a.astype(F32), choice_b.astype(F32), wts[...], jnp.zeros((4, tb), F32)], axis=0
    ).T
    q = iota((tb, slots), 1)
    expert = (lax.div(q, 16) * GROUPS + lax.div(lax.rem(q, 16), 2)).astype(F32)
    hit_a = jnp.where(lines[:, 0:1] == expert, 1.0, 0.0)
    hit_b = jnp.where(lines[:, 1:2] == expert, 1.0, 0.0)
    earlier = jnp.where(iota((tb, tb), 0) > iota((tb, tb), 1), 1.0, 0.0).astype(BF16)
    rank = nn(earlier, (hit_a + hit_b).astype(BF16))
    weight = jnp.where(
        rank == lax.rem(q, 2).astype(F32), hit_a * lines[:, 2:3] + hit_b * lines[:, 3:4], 0.0
    )

    pair_shared.wait()
    ss[...] = (sp[c].astype(F32) + spr[...].astype(F32)).astype(BF16)
    sb[y] = ss[y]
    y_sends = []
    for k, d in enumerate(FAR_FIRST):
        to = lax.rem(y + d, GROUPS)
        y_sends.append(
            remote(ss.at[to], sb.at[y], ysend.at[k], yrecv.at[k], {"tp": 2 * to + c})
        )
        y_sends[-1].start()

    for copy in x_sends:
        copy.wait()
    stretch = [xarr[k] for k in range(nx)]
    level = stretch
    while len(level) > 1:
        pairs = [joined(level[k + 1], level[k]) for k in range(0, len(level) - 1, 2)]
        level = pairs + [v.astype(F32) for v in level[2 * len(pairs) :]]
    total = level[0]
    zs[...] = total.astype(BF16)
    for d in range(1, nz):
        @pl.when(z + d < nz)
        def _():
            remote(
                zs, zarr.at[z], zsend.at[d - 1], zrecv.at[z], {"ep": (z + d) * nx + x}
            ).start()

    before, upto = unit, stretch[0].astype(F32)
    for k in range(1, nx):
        before = jnp.where(x == k, upto, before)
        if k < nx - 1:
            upto = joined(stretch[k], upto)
    zsc[...] = mm(beside_identity(before).T, z_all)

    order = FAR_FIRST + (0,)
    middle = aps.shape[2] // 2
    halves = (slice(0, middle), slice(middle, 2 * middle))

    def ring(step, way, part):
        k = 3 * way + step
        to = lax.rem(y + (GROUPS - 1 if way else 1), GROUPS)
        slot = order.index(4 + step if way else 3 - step)
        return remote(
            aps.at[slot, :, halves[part]], ring_in.at[k, :, halves[part]],
            rsum_s.at[part, k], rsum_r.at[part, k], {"tp": 2 * to + c},
        )

    def ring_on(step):
        for part in range(2):
            for way in range(2):
                if step < 3 + way:
                    ring(step - 1, way, part).wait_recv()
                    slot = order.index(4 + step if way else 3 - step)
                    arrived = ring_in[3 * way + step - 1, :, halves[part]].astype(F32)
                    kept = aps[slot, :, halves[part]].astype(F32)
                    aps[slot, :, halves[part]] = (kept + arrived).astype(BF16)
                    ring(step, way, part).start()

    def heads():
        for k in range(nz - 1):
            @pl.when(k < z)
            def _():
                drain(zarr.at[k], zrecv.at[k])

        level = [zarr[k] for k in range(nz - 1)] if nz > 1 else [unit.astype(BF16)]
        while len(level) > 1:
            nxt = [joined(level[k + 1], level[k]) for k in range(0, len(level) - 1, 2)]
            if len(level) % 2:
                nxt.append(level[-1].astype(F32))
            level = nxt

        carried = level[0].astype(F32)
        head = mm(beside_identity(carried).T[:HC], zsc[...])
        centred = head - jnp.mean(head, axis=0, keepdims=True)
        normed = centred * lax.rsqrt(jnp.mean(centred * centred, axis=0, keepdims=True) + GROUP_EPSILON)
        heads_out = normed * column(hng[...]) * sigmoid(gat[...].astype(F32))
        heads_out = heads_out.T.astype(BF16)
        own_rows = out_a.shape[0]
        ho[...] = heads_out.reshape(GROUPS, 2, own_rows, HC)

    def project():
        own_rows = out_a.shape[0]
        ready(19, 20)

        half = GROUPS // 2

        def product(first, core):
            lines = [ho[lax.rem(y + d, GROUPS), core] for d in order[first : first + half]]
            return nn(jnp.concatenate(lines, axis=0), how[...])

        pair_mix = []
        for k in range(2):
            at = slice(k * half, (k + 1) * half)
            ap[at] = product(k * half, 1 - c).astype(BF16).reshape(half, own_rows, -1)
            pair_mix.append(
                remote(ap.at[at], apr.at[at], pair_s.at[2 + k], pair_r.at[2 + k], {"tp": other})
            )
            pair_mix[-1].start()
        mixed = [product(k * half, c).astype(BF16).astype(F32) for k in range(2)]

        for k in range(2):
            at = slice(k * half, (k + 1) * half)
            pair_mix[k].wait()
            aps[at] = (mixed[k].reshape(half, own_rows, -1) + apr[at].astype(F32)).astype(BF16)
            if k == 0:
                for part in range(2):
                    for way in range(2):
                        ring(0, way, part).start()

    @pl.when(z < nz // 2)
    def _():
        heads()
        project()

    drain(darr.at[c, 0 : n_ep - 1], drecv)
    pair_rows = remote(darr.at[c], darr.at[c], pair_s.at[4], pair_r.at[4], {"tp": other})
    pair_rows.start()
    pair_rows.wait()

    rows_in = jnp.concatenate([darr[h].reshape(rows, width) for h in range(2)], axis=1)
    ready(16, 18)
    g, u = nn(rows_in, rg[...]), nn(rows_in, ru[...])
    hidden = (g * sigmoid(g) * u).astype(BF16)
    ready(18, 19)
    routed = nn(hidden, rd[...]).astype(BF16)
    for k in range(2 * GROUPS):
        ep[k % 2, k // 2] = routed[:, k * cols : (k + 1) * cols]
    pair_routed = remote(ep.at[1 - c], epr, pair_s.at[1], pair_r.at[1], {"tp": other})
    pair_routed.start()

    @pl.when(z < nz // 2)
    def _():
        ring_on(1)

    @pl.when(z >= nz // 2)
    def _():
        heads()

    pair_routed.wait()
    both = ep[c].astype(F32) + epr[...].astype(F32)
    es[...] = both.reshape(GROUPS * n_ep, CAP, cols).astype(BF16)
    place = me * GROUPS + y
    rarr[place] = es[y * n_ep + me]
    pl.semaphore_wait(seen, GROUPS - 1)

    def send_back(k, carry):
        yo = lax.rem(y + GROUPS // 2 + k, GROUPS)
        for zo, xo in offsets():
            to = lax.rem(z + zo, nz) * nx + lax.rem(x + xo, nx)
            copy = remote(
                es.at[yo * n_ep + to], rarr.at[place], rsend, rrecv, {"ep": to, "tp": 2 * yo + c}
            )
            if zo or xo:
                copy.start()
            else:
                pl.when(yo != y)(copy.start)
        return carry

    lax.fori_loop(0, GROUPS, send_back, 0)

    @pl.when(z >= nz // 2)
    def _():
        project()

    @pl.when(z >= nz // 2)
    def _():
        ring_on(1)

    ring_on(2)
    ring_on(3)

    ready(20, 21)
    for part in range(2):
        ring(2, 0, part).wait_recv()
        ring(3, 1, part).wait_recv()
    mix = aps[GROUPS - 1].astype(F32) + ring_in[2].astype(F32) + ring_in[6].astype(F32)
    scale = lax.rsqrt(jnp.mean(mix * mix, axis=1, keepdims=True) + NORM_EPSILON)
    out_a[...] = (mix * scale * png[...]).astype(BF16)

    for copy in y_sends:
        copy.wait()
    drain(rarr.at[0 : n_ep * GROUPS - 1], rrecv)
    answer = mm(weight, rarr[...].reshape(slots, cols))
    for k in range(GROUPS):
        answer = answer + sb[k].astype(F32)
    out_b[...] = answer.astype(BF16)


    for d in range(1, nz):
        @pl.when(z + d < nz)
        def _():
            drain(zs, zsend.at[d - 1])
    for way in range(2):
        for step in range(3 + way):
            for part in range(2):
                ring(step, way, part).wait_send()
    drain(dout.at[0 : n_ep - 1], dsend)
    drain(es.at[0 : n_ep * GROUPS - 1], rsend)


def solution(mesh):
    n_ep = mesh.shape["ep"]
    nx = 4 if n_ep % 4 == 0 else n_ep
    nz = n_ep // nx

    def body(rec, key, val, dec, lrn, gat, dco, spk, hng, how, png, exr, eng, idx, wts,
             rg, ru, rd, cg, cu, cd):
        ta, d = rec.shape[0], how.shape[1]
        tb = exr.shape[0]
        own, cols = ta // (2 * GROUPS), d // (2 * GROUPS)
        rows = n_ep * CAP
        line = lambda a: a.reshape(1, -1)
        given = [
            exr, line(eng), idx.T, cg.T, cu.T, cd, rec.T, key.T, val.T, dec.T, lrn.T, spk.T,
            line(dco), gat.T, line(hng), wts.T, rg[0], ru[0], rd[0], how, line(png),
        ]
        held = [pltpu.VMEM(a.shape, a.dtype) for a in given]
        held[3:5] = [pltpu.VMEM((2 * HC, d), BF16)]
        hbm = pl.BlockSpec(memory_space=pltpu.HBM)
        vmem = pl.BlockSpec(memory_space=pltpu.VMEM)
        given = [pltpu.with_memory_space_constraint(a, pltpu.HBM) for a in given]
        dma = pltpu.SemaphoreType.DMA
        return pl.pallas_call(
            functools.partial(kernel, nx, nz),
            out_shape=(
                jax.ShapeDtypeStruct((own, d), BF16),
                jax.ShapeDtypeStruct((tb, cols), BF16),
            ),
            in_specs=[hbm] * len(given),
            out_specs=(vmem, vmem),
            scratch_shapes=[
                *held,
                pltpu.VMEM((tb, d), BF16),
                pltpu.VMEM((n_ep, CAP, d // 2), BF16),
                pltpu.VMEM((2, n_ep, CAP, d // 2), BF16),
                pltpu.VMEM((2, GROUPS, rows, cols), BF16),
                pltpu.VMEM((GROUPS, rows, cols), BF16),
                pltpu.VMEM((GROUPS * n_ep, CAP, cols), BF16),
                pltpu.VMEM((GROUPS * n_ep, CAP, cols), BF16),
                pltpu.VMEM((2, GROUPS, tb, cols), BF16),
                pltpu.VMEM((GROUPS, tb, cols), BF16),
                pltpu.VMEM((GROUPS, tb, cols), BF16),
                pltpu.VMEM((GROUPS, tb, cols), BF16),
                pltpu.VMEM((GROUPS, 2, own, HC), BF16),
                pltpu.VMEM((GROUPS, own, d), BF16),
                pltpu.VMEM((GROUPS, own, d), BF16),
                pltpu.VMEM((GROUPS, own, d), BF16),
                pltpu.VMEM((GROUPS - 1, own, d), BF16),
                pltpu.VMEM((nx, HC, 2 * HC), BF16),
                pltpu.VMEM((HC, 2 * HC), BF16),
                pltpu.VMEM((nz, HC, 2 * HC), BF16),
                dma((len(given),)),
                dma((5,)),
                dma((5,)),
                dma,
                dma,
                pltpu.SemaphoreType.REGULAR,
                dma((GROUPS - 1,)),
                dma((GROUPS - 1,)),
                dma((2, 7)),
                dma((2, 7)),
                dma,
                dma,
                dma((max(nx - 1, 1),)),
                dma((max(nx - 1, 1),)),
                dma((max(nz - 1, 1),)),
                dma((max(nz, 1),)),
                pltpu.VMEM((2 * HC, ta), F32),
            ],
            compiler_params=pltpu.CompilerParams(
                collective_id=0, has_side_effects=True, vmem_limit_bytes=48 * 1024 * 1024
            ),
        )(*given)

    placed = (
        P("ep", "tp"), P("ep", "tp"), P("ep", "tp"), P("ep", "tp"), P("ep", "tp"), P("ep", "tp"),
        P("tp"), P("ep", "tp"), P("tp"), P("tp", None), P(), P("ep", None), P(), P("ep", None),
        P("ep", None), P(("ep", "tp"), None, None), P(("ep", "tp"), None, None),
        P(("ep", "tp"), None, None), P(None, "tp"), P(None, "tp"), P("tp", None),
    )
    return jax.shard_map(
        body,
        mesh=mesh,
        in_specs=placed,
        out_specs=(P(("ep", "tp"), None), P("ep", "tp")),
        check_vma=False,
    )
```
